512 devices in a mesh: grp: 2 (over y), kv: 64 (over z, core), tp: 4 (over x).
Axes of the slice: x: 4, y: 2, z: 32, core: 2. Of those that a mesh axis runs over, the one named last changes fastest.
The devices are a block of a 4x8x32 slice.
Arguments:
- tokens: bfloat16 [128, 3, 4096], P(('grp', 'kv')), parts along dimension 0, may hold values from -6 to 6
- input_norm_scale: float32 [4096], replicated, may hold values from 0.1 to 1.9
- head_input_matrix: bfloat16 [4096, 8192], P('kv', 'tp'), may hold values from -0.09375 to 0.09375
- output_gate_matrix: bfloat16 [4096, 8192], P('kv', 'tp'), may hold values from -0.09375 to 0.09375
- group_input_matrix: bfloat16 [4096, 512], P('kv', 'tp'), may hold values from -0.09375 to 0.09375
- group_readout_matrix: bfloat16 [4096, 512], P('kv', 'tp'), may hold values from -0.09375 to 0.09375
- step_size_matrix: bfloat16 [4096, 128], P(None, 'tp'), may hold values from -0.09375 to 0.09375
- step_size_bias: float32 [128], P('tp'), may hold values from -4 to -1
- log_decay_rate: float32 [128], P('tp'), may hold values from -4.6 to 2
- direct_path_weight: float32 [128], P('tp'), may hold values from 0.1 to 1.9
- convolution_tap_weight: bfloat16 [4, 8, 1152], P(None, 'tp'), may hold values from -3 to 3
- convolution_history_rows: bfloat16 [128, 6, 8, 1152], P(('grp', 'kv'), None, 'tp'), parts along dimension 0, may hold values from -6 to 6
- per_proposal_states: float32 [128, 3, 128, 64, 64], P(('grp', 'kv'), None, 'tp'), parts along dimension 0, may hold values from -4 to 4
- accepted: int32 [128], P(('grp', 'kv')), parts along dimension 0, may hold values from 1 to 3
- proposal_extra_decay: float32 [128, 3, 128], P(('grp', 'kv'), None, 'tp'), parts along dimension 0, may hold values from -0.69 to 0
- group_norm_scale: float32 [8192], P('tp'), may hold values from 0.1 to 1.9
- output_projection_matrix: bfloat16 [8192, 4096], P('tp', 'kv'), may hold values from -0.0625 to 0.0625
Outputs:
- mixed: bfloat16 [128, 3, 4096], P(('grp', 'tp'), None, 'kv'), parts along dimension 0
- new_states: float32 [128, 3, 128, 64, 64], P(('grp', 'kv'), None, 'tp'), parts along dimension 0
- new_tail: bfloat16 [128, 6, 8, 1152], P(('grp', 'kv'), None, 'tp'), parts along dimension 0
The draws below stay inside these ranges and needn't reach their ends.
There are 2 independent parts, one for each index of `grp`. The reference program is written for one: setup_inputs(seed, part) draws one part's arguments, and reference() takes and returns one part's arrays. A program takes and returns all parts, laid end to end along the dimension named above; an argument that names none is the same for every part. Nothing has to cross between parts.
All inputs are finite; a program needn't handle non-finite values.
Results may differ from the reference program's by a relative error of at most 0.015.
Values may be sent and summed in bfloat16 or wider, within the bound.
A program may use at most 64 MiB of HBM per device.

```python
import jax
import jax.numpy as jnp
from jax import lax

D = 4096
HEADS = 128
HEAD_DIM = 64
GROUPS = 8
STATE = 64
CONV_W = 4
PROP = 3
SEQS = 64
GROUP_CH = 1152
TAIL = 6
N_TP = 4


def draw_proposal_extra_decay(key, part):
    first_key, second_key = jax.random.split(jax.random.fold_in(key, 11))
    struck = jax.random.uniform(first_key, (SEQS, PROP, HEADS), jnp.float32) < 0.15
    depth = jax.random.uniform(second_key, (SEQS, PROP, HEADS), jnp.float32, 0.22, 0.69)
    return jnp.where(struck, -depth, 0.0).astype(jnp.float32)


def touch_ends(result, stream_key, least, largest):
    longest = result.shape.index(max(result.shape))
    spots = []
    for shift in (0, 1):
        where = [jax.random.randint(jax.random.fold_in(stream_key, axis), (), 0, length) for axis, length in enumerate(result.shape)]
        where[longest] = (where[longest] + shift) % result.shape[longest]
        spots.append(tuple(where))
    return result.at[spots[0]].set(least).at[spots[1]].set(largest)


def block_scale(stream_key, extent, pieces, smallest, top_value):
    level, own = 1.0, jax.random.fold_in(stream_key, 6)
    for axis_at, parts in pieces:
        heights = jnp.exp(jax.random.uniform(jax.random.fold_in(own, axis_at), (parts,), jnp.float32, smallest / len(pieces), top_value / len(pieces)))
        level = level * jnp.repeat(heights, extent[axis_at] // parts).reshape([-1 if axis == axis_at else 1 for axis in range(len(extent))])
    return level


def noise(rng, extent, deviation, reach, cuts=(), kind=jnp.bfloat16):
    gain = block_scale(rng, extent, cuts, -0.22, 0.18) if cuts else 1.0
    entries = jax.random.normal(rng, extent, jnp.float32) * deviation * gain
    return jnp.minimum(jnp.maximum(entries, -reach), reach).astype(kind)


def setup_inputs(seed: int = 0, part: int = 0) -> dict:
    key_of = jax.random.split(jax.random.key(seed), 18)
    part_splits = jax.random.split(jax.random.fold_in(key_of[17], part), 18)
    tokens = noise(part_splits[0], (SEQS, PROP, D), 1.0, 6.0, ((0, 64),))
    input_norm_scale = jnp.clip(1.0 + 0.18 * jax.random.normal(key_of[1], (D,), jnp.float32), 0.1, 1.9)
    head_input_matrix = noise(key_of[2], (D, HEADS * HEAD_DIM), D ** -0.5, 0.09375, ((0, 64), (1, 4)))
    output_gate_matrix = noise(key_of[3], (D, HEADS * HEAD_DIM), D ** -0.5, 0.09375, ((0, 64), (1, 4)))
    group_input_matrix = noise(key_of[4], (D, GROUPS * STATE), D ** -0.5, 0.09375, ((0, 64), (1, 4)))
    group_readout_matrix = noise(key_of[5], (D, GROUPS * STATE), D ** -0.5, 0.09375, ((0, 64), (1, 4)))
    step_size_matrix = noise(key_of[6], (D, HEADS), D ** -0.5, 0.09375, ((1, 4),))
    step_size_bias = jnp.clip(-4.0 + 3.0 * jax.random.uniform(key_of[7], (HEADS,), jnp.float32) ** block_scale(key_of[7], (HEADS,), ((0, 4),), -0.2, 0.2), -4.0, -1.0)
    log_decay_rate = jnp.clip(-4.6 + 6.6 * jax.random.uniform(key_of[8], (HEADS,), jnp.float32) ** block_scale(key_of[8], (HEADS,), ((0, 4),), -0.2, 0.2), -4.6, 2.0)
    direct_path_weight = jnp.clip(1.0 + 0.18 * jax.random.normal(key_of[9], (HEADS,), jnp.float32), 0.1, 1.9)
    convolution_tap_weight = noise(key_of[10], (CONV_W, GROUPS, GROUP_CH), 0.5, 3.0, ((1, 4),))
    convolution_history_rows = noise(part_splits[11], (SEQS, TAIL, GROUPS, GROUP_CH), 1.0, 6.0, ((0, 64), (2, 4)))
    per_proposal_states = noise(part_splits[12], (SEQS, PROP, HEADS, HEAD_DIM, STATE), 0.5, 4.0, ((0, 64), (2, 4)), jnp.float32)
    accepted = touch_ends(jax.random.randint(part_splits[13], (SEQS,), 1, PROP + 1), jax.random.fold_in(part_splits[13], 1), 1, PROP).astype(jnp.int32)
    proposal_extra_decay = draw_proposal_extra_decay(jax.random.fold_in(jax.random.fold_in(key_of[17], part), 71), part)
    group_norm_scale = jnp.clip(1.0 + 0.18 * jax.random.normal(key_of[15], (HEADS * HEAD_DIM,), jnp.float32), 0.1, 1.9)
    output_projection_matrix = noise(key_of[16], (HEADS * HEAD_DIM, D), (HEADS * HEAD_DIM) ** -0.5, 0.0625, ((0, 4), (1, 64)))
    return {"tokens": tokens, "input_norm_scale": input_norm_scale, "head_input_matrix": head_input_matrix, "output_gate_matrix": output_gate_matrix, "group_input_matrix": group_input_matrix, "group_readout_matrix": group_readout_matrix, "step_size_matrix": step_size_matrix, "step_size_bias": step_size_bias, "log_decay_rate": log_decay_rate, "direct_path_weight": direct_path_weight, "convolution_tap_weight": convolution_tap_weight, "convolution_history_rows": convolution_history_rows, "per_proposal_states": per_proposal_states, "accepted": accepted, "proposal_extra_decay": proposal_extra_decay, "group_norm_scale": group_norm_scale, "output_projection_matrix": output_projection_matrix}


epsilon = 1e-06

def rms_scale(values):
    return lax.rsqrt(lax.optimization_barrier(jnp.mean(values * values, axis=-1, keepdims=True)) + epsilon)

def causal_states(log_decay_factor, head_step_size, ssm_inputs, inject, start_state):
    cumulative = jnp.cumsum(log_decay_factor, axis=1)
    length = log_decay_factor.shape[1]
    lower = (jnp.arange(length)[:, None] >= jnp.arange(length)[None, :])[None, :, :, None]
    spread = cumulative[:, :, None, :] - cumulative[:, None, :, :]
    factors = jnp.where(lower, jnp.exp(jnp.where(lower, spread, 0.0)), 0.0)
    mixing = factors * head_step_size[:, None, :, :]
    carried = jnp.exp(cumulative)[..., None, None] * start_state[:, None]
    return carried + jnp.einsum('sjih,sihp,sihn->sjhpn', mixing, ssm_inputs, inject)

def combine_head_outputs(incoming_token_rows, gate_portion, unactivated_step, step_size_bias, log_decay_rate, direct_path_weight, convolution_tap_weight, convolution_history_rows, per_proposal_states, accepted, proposal_extra_decay, group_norm_scale):
    sequences, proposals, group_count, group_width = incoming_token_rows.shape
    head_count = step_size_bias.shape[0]
    head_dim = per_proposal_states.shape[3]
    state_size = per_proposal_states.shape[4]
    per_group = head_count // group_count
    group_inner = per_group * head_dim
    tap_count = convolution_tap_weight.shape[0]
    offsets = accepted[:, None] + jnp.arange(tap_count - 1, dtype=jnp.int32)[None, :]
    context = jnp.take_along_axis(convolution_history_rows, offsets[:, :, None, None], axis=1)
    convolution_span = jnp.concatenate([context, incoming_token_rows], axis=1)
    widened = convolution_span.astype(jnp.float32)
    convolved = jnp.zeros((sequences, proposals, group_count, group_width), jnp.float32)
    for conv_tap in range(tap_count):
        convolved = convolved + widened[:, conv_tap:conv_tap + proposals] * convolution_tap_weight[conv_tap].astype(jnp.float32)
    activated = jax.nn.silu(convolved)
    ssm_inputs = activated[..., :group_inner].reshape(sequences, proposals, head_count, head_dim)
    inject = jnp.repeat(activated[..., group_inner:group_inner + state_size], per_group, axis=2)
    readout = jnp.repeat(activated[..., group_inner + state_size:], per_group, axis=2)
    head_step_size = jax.nn.softplus(unactivated_step + step_size_bias)
    log_decay_factor = proposal_extra_decay - jnp.exp(log_decay_rate) * head_step_size
    chosen = (accepted - 1)[:, None, None, None, None]
    start_state = jnp.take_along_axis(per_proposal_states, chosen, axis=1)[:, 0]
    running_state_rows = causal_states(log_decay_factor, head_step_size, ssm_inputs, inject, start_state)
    response = jnp.einsum('sjhn,sjhpn->sjhp', readout, running_state_rows) + direct_path_weight[:, None] * ssm_inputs
    gate_raw = gate_portion.astype(jnp.float32).reshape(sequences, proposals, head_count, head_dim)
    gate_applied_output = (response * jax.nn.silu(gate_raw)).reshape(sequences, proposals, group_count, group_inner)
    scaled = gate_applied_output * rms_scale(gate_applied_output) * group_norm_scale.reshape(group_count, group_inner)
    flat_gated = scaled.astype(jnp.bfloat16).reshape(sequences, proposals, head_count * head_dim)
    return (flat_gated, running_state_rows, convolution_span)

def reference(tokens, input_norm_scale, head_input_matrix, output_gate_matrix, group_input_matrix, group_readout_matrix, step_size_matrix, step_size_bias, log_decay_rate, direct_path_weight, convolution_tap_weight, convolution_history_rows, per_proposal_states, accepted, proposal_extra_decay, group_norm_scale, output_projection_matrix):
    widened = tokens.astype(jnp.float32)
    normed = (widened * rms_scale(widened) * input_norm_scale).astype(jnp.bfloat16)
    flattened = normed.reshape(SEQS * PROP, D)

    def project(weight):
        return jnp.dot(flattened, weight, preferred_element_type=jnp.float32).astype(jnp.bfloat16)
    per_group = HEADS // GROUPS
    part_input = project(head_input_matrix).reshape(SEQS, PROP, GROUPS, per_group * HEAD_DIM)
    part_inject = project(group_input_matrix).reshape(SEQS, PROP, GROUPS, STATE)
    part_readout = project(group_readout_matrix).reshape(SEQS, PROP, GROUPS, STATE)
    gate_portion = project(output_gate_matrix).reshape(SEQS, PROP, HEADS * HEAD_DIM)
    unactivated_step = jnp.dot(flattened, step_size_matrix, preferred_element_type=jnp.float32).reshape(SEQS, PROP, HEADS)
    incoming_token_rows = jnp.concatenate([part_input, part_inject, part_readout], axis=-1)
    gate_applied_output, running_state_rows, convolution_span = combine_head_outputs(incoming_token_rows, gate_portion, unactivated_step, step_size_bias, log_decay_rate, direct_path_weight, convolution_tap_weight, convolution_history_rows, per_proposal_states, accepted, proposal_extra_decay, group_norm_scale)
    block_width = HEADS * HEAD_DIM // N_TP
    gathered = gate_applied_output.reshape(SEQS * PROP, HEADS * HEAD_DIM)
    total = jnp.zeros((SEQS * PROP, D), jnp.float32)
    for shard in range(N_TP):
        partial_sum = jnp.dot(gathered[:, shard * block_width:(shard + 1) * block_width], output_projection_matrix[shard * block_width:(shard + 1) * block_width], preferred_element_type=jnp.float32)
        total = total + lax.optimization_barrier(partial_sum.astype(jnp.bfloat16)).astype(jnp.float32)
    mixed = total.astype(jnp.bfloat16).reshape(SEQS, PROP, D)
    return (mixed, running_state_rows, convolution_span)
```

```python
import functools

import jax
import jax.numpy as jnp
from jax import lax
from jax.experimental import pallas as pl
from jax.experimental.pallas import tpu as pltpu
from jax.sharding import Mesh
from jax.sharding import PartitionSpec as P

MESH = pl.DeviceIdType.MESH
EPS = 1e-06
F32 = jnp.float32
BF16 = jnp.bfloat16

KV = ("z", "c")
GRP_KV = ("grp", "z", "c")

NZ = 32
BLK = 896
CB = 5
GBLK = 384


def iota(shape, dim):
    return lax.broadcasted_iota(jnp.int32, shape, dim)


def split3(v):
    hi = v.astype(BF16)
    rest = v - hi.astype(F32)
    mid = rest.astype(BF16)
    lo = (rest - mid.astype(F32)).astype(BF16)
    return hi, mid, lo


def dot(a, b):
    return jnp.dot(a, b, preferred_element_type=F32)


def dot_nt(a, b):
    return lax.dot_general(a, b, (((1,), (1,)), ((), ())), preferred_element_type=F32)


def dot_tn(a, b):
    return lax.dot_general(a, b, (((0,), (0,)), ((), ())), preferred_element_type=F32)


def silu(v):
    return v / (1.0 + jnp.exp(-v))


def one_hot(cond):
    return jnp.where(cond, 1.0, 0.0).astype(BF16)


PIECES = (
    (0, 0, 896, 0, 0),
    (0, 896, 896, 1, 0),
    (0, 1792, 256, 2, 0),
    (2, 0, 128, 2, 256),
    (3, 0, 128, 2, 384),
    (1, 0, 384, 2, 512),
    (1, 384, 896, 3, 0),
    (1, 1280, 768, 4, 0),
)


def kernel(
    tok_h, ins_h, wh_h, wg_h, wi_h, wr_h, ws_h, bias_h, ldr_h, dpw_h, tap_h, hist_h, st_h, acc_s, ped_h, gns_h, wo_h,
    mixed_o, states_o, tail_o,
    tok, ins, ws, bias, ldr, dpw, tap, hist, st, ped, gns, wo, wop,
    w2, nst, xs, part, mem, cout, cin, gath, gown, fin, fst, snew, s0cat, span_v,
    lsem, wsend, wrecv, asend, arecv, msend, mrecv, csend, crecv, gsend, grecv, nrecv, fsend, frecv, osem,
):
    z = lax.axis_index("z")
    c = lax.axis_index("c")
    t = lax.axis_index("tp")
    n_tp = lax.axis_size("tp")

    def at(offset):
        return lax.rem(z + (offset + NZ) % NZ, NZ)

    barrier = pltpu.get_barrier_semaphore()

    def greet(k, _):
        pl.semaphore_signal(barrier, inc=1, device_id={"z": lax.rem(z + k, NZ)}, device_id_type=MESH)
        return 0

    lax.fori_loop(1, NZ, greet, 0)
    others = [(dc, dt) for dc in range(2) for dt in range(n_tp) if (dc, dt) != (0, 0)]
    for dc, dt in others:
        pl.semaphore_signal(
            barrier, inc=1, device_id={"c": lax.rem(c + dc, 2), "tp": lax.rem(t + dt, n_tp)}, device_id_type=MESH
        )

    pairs = [
        (tok_h.at[0], tok), (ins_h, ins), (ws_h, ws), (bias_h, bias), (ldr_h, ldr), (dpw_h, dpw), (tap_h, tap),
        (hist_h.at[0], hist), (ped_h.at[0], ped), (gns_h, gns), (st_h, st), (wo_h, wo),
    ]
    loads = [pltpu.make_async_copy(src, dst, lsem.at[i]) for i, (src, dst) in enumerate(pairs)]
    sources = (wh_h, wg_h, wi_h, wr_h)
    mine = pl.multiple_of(c * 64, 64)
    for i, (source, first, count, row, lane) in enumerate(PIECES):
        loads.append(
            pltpu.make_async_copy(
                sources[source].at[:, first : first + count],
                w2.at[pl.ds(pl.multiple_of(row * 128 + mine, 64), 64), lane : lane + count],
                lsem.at[len(pairs) + i],
            )
        )
    for cp in loads:
        cp.start()

    loads[0].wait()
    loads[1].wait()
    wide = tok[...].astype(F32)
    scale = lax.rsqrt(jnp.sum(wide * wide, axis=-1, keepdims=True) * (1.0 / wide.shape[1]) + EPS)
    normed = (wide * scale * ins[...]).astype(BF16)
    row16 = iota((16, 3), 0)
    spread = one_hot((row16 // CB == iota((16, 3), 1)) & (row16 < 3 * CB))
    sent = dot(spread, normed).astype(BF16)
    for k in range(NZ):
        nst[k] = sent[:, k * 128 : (k + 1) * 128]

    pl.semaphore_wait(barrier, NZ - 1 + len(others))

    def send_slice(k, _):
        to = lax.rem(z + k, NZ)
        pltpu.make_async_remote_copy(
            src_ref=nst.at[to], dst_ref=xs.at[z], send_sem=asend, recv_sem=arecv, device_id={"z": to}, device_id_type=MESH
        ).start()
        return 0

    lax.fori_loop(1, NZ, send_slice, 0)
    xs[z] = nst[z]

    partner = {"c": 1 - c}
    shares = []
    for i, (source, first, count, row, lane) in enumerate(PIECES):
        shares.append(
            pltpu.make_async_remote_copy(
                src_ref=sources[source].at[:, first : first + count],
                dst_ref=w2.at[pl.ds(pl.multiple_of(row * 128 + mine, 64), 64), lane : lane + count],
                send_sem=wsend.at[i], recv_sem=wrecv.at[i], device_id=partner, device_id_type=MESH,
            )
        )
    shares.append(
        pltpu.make_async_remote_copy(
            src_ref=wo_h, dst_ref=wop, send_sem=wsend.at[len(PIECES)], recv_sem=wrecv.at[len(PIECES)],
            device_id=partner, device_id_type=MESH,
        )
    )
    for cp in shares:
        cp.start()

    for cp in loads[2:]:
        cp.wait()
    w2[4 * 128 :, 768:] = jnp.zeros((128, 128), BF16)
    step_raw = dot(normed, ws[...])
    raw = step_raw + bias[...]
    step = jnp.maximum(raw, 0.0) + jnp.log1p(jnp.exp(-jnp.abs(raw)))
    decay = ped[...] - jnp.exp(ldr[...]) * step
    cum0 = decay[0:1]
    cum1 = cum0 + decay[1:2]
    cum2 = cum1 + decay[2:3]
    none = jnp.zeros_like(cum0)
    zeros5 = jnp.zeros((5, cum0.shape[1]), F32)

    def rows(a, b, d):
        return jnp.concatenate([a, b, d, zeros5], axis=0)

    per_head = jnp.concatenate(
        [
            rows(jnp.exp(cum0), jnp.exp(cum1), jnp.exp(cum2)),
            rows(step[0:1], step[1:2], step[2:3]),
            rows(none, jnp.exp(cum1 - cum0) * step[0:1], jnp.exp(cum2 - cum1) * step[1:2]),
            rows(none, none, jnp.exp(cum2 - cum0) * step[0:1]),
            rows(dpw[...], dpw[...], dpw[...]),
        ],
        axis=0,
    )
    heads = per_head.shape[1]
    lanes = heads * 64
    to_head = iota((heads, lanes), 1) - iota((heads, lanes), 0) * 64
    expand = one_hot((to_head >= 0) & (to_head < 64))
    hi, mid, lo = split3(per_head)
    wide_heads = dot(hi, expand) + dot(mid, expand) + dot(lo, expand)
    carry_w, mix0, mix1, mix2, direct = (wide_heads[i * 8 : (i + 1) * 8] for i in range(5))

    start = jnp.clip(acc_s[0] - 1, 0, 2)
    ones3 = jnp.ones((3, 64), BF16)
    for g in range(2):
        at_g = slice(g * 1024, (g + 1) * 1024)
        s0 = st[start, at_g, :]
        s_hi = s0.astype(BF16)
        s_lo = (s0 - s_hi.astype(F32)).astype(BF16)
        s0cat[at_g, :] = jnp.concatenate([s_hi, s_lo], axis=1)
        for j in range(3):
            line = carry_w[j : j + 1, at_g]
            l_hi, l_mid, l_lo = split3(line)
            stack = jnp.concatenate([l_hi.astype(F32), l_mid.astype(F32), l_lo.astype(F32)], axis=0).astype(BF16)
            snew[j, at_g, :] = dot_tn(stack, ones3) * s0

    def in_order(v):
        a, b = v[:, 0, :], v[:, 1, :]
        return jnp.concatenate(
            [a[:, :1024], b[:, :1024], a[:, 1024:1088], b[:, 1024:1088], a[:, 1088:], b[:, 1088:]], axis=1
        )

    kept = in_order(hist[...].astype(F32))
    taps = in_order(tap[...].astype(F32))
    accepted = acc_s[0]
    context = jnp.where(accepted == 1, kept[1:4], jnp.where(accepted == 2, kept[2:5], kept[3:6]))
    context = jnp.concatenate([context, jnp.zeros((5, context.shape[1]), F32)], axis=0)

    for cp in shares:
        cp.wait_recv()
    pltpu.make_async_remote_copy(
        src_ref=nst.at[0 : NZ - 1], dst_ref=xs.at[0 : NZ - 1], send_sem=asend, recv_sem=arecv, device_id=partner,
        device_id_type=MESH,
    ).wait_recv()
    x_all = xs[...].reshape(NZ * 16, 128)
    block_of = lax.rem(lax.rem(iota((NZ * 16, 128), 0), 16), CB)
    zero = jnp.zeros_like(x_all)
    stacked = jnp.concatenate([jnp.where(block_of == cb, x_all, zero) for cb in range(CB)], axis=1)
    for n0, n1 in ((0, 256), (256, 512), (512, 768), (768, 896)):
        part[:, :, n0:n1] = dot(stacked, w2[:, n0:n1]).astype(BF16).reshape(NZ, 16, n1 - n0)

    def member(delta, hop, head, slot):
        pltpu.make_async_remote_copy(
            src_ref=part.at[at(delta)], dst_ref=mem.at[head // 4, slot], send_sem=msend, recv_sem=mrecv.at[head // 4],
            device_id={"z": at(hop)}, device_id_type=MESH,
        ).start()

    def members(head):
        member((head + 1) % NZ, 1, head, 0)
        member((head - 1) % NZ, -1, head, 1)
        if head < 16:
            member(head + 2, 2, head, 2)
        if head > 16:
            member(head - 2, -2, head, 2)
        if head == 0:
            member(NZ - 2, -2, head, 3)

    def quad(head):
        count = {0: 4, 16: 2}.get(head, 3)
        pltpu.make_async_remote_copy(
            src_ref=mem.at[head // 4, 0:count], dst_ref=mem.at[head // 4, 0:count], send_sem=msend,
            recv_sem=mrecv.at[head // 4], device_id=partner, device_id_type=MESH,
        ).wait_recv()
        total = part[at(head)].astype(F32)
        for slot in range(count):
            total += mem[head // 4, slot].astype(F32)
        return total

    def chain(step_at, hop):
        return pltpu.make_async_remote_copy(
            src_ref=cout.at[step_at], dst_ref=cin.at[step_at], send_sem=csend.at[step_at], recv_sem=crecv.at[step_at],
            device_id={"z": at(hop)}, device_id_type=MESH,
        )

    right = [chain(i, 4) for i in range(4)]
    left = [chain(4 + i, -4) for i in range(3)]
    for head in (16, 12, 20):
        members(head)
    cout[0] = quad(16).astype(BF16)
    right[0].start()
    cout[4] = quad(20).astype(BF16)
    left[0].start()
    for head in (8, 24):
        members(head)
    total = quad(12)
    right[0].wait_recv()
    cout[1] = (total + cin[0].astype(F32)).astype(BF16)
    right[1].start()
    total = quad(24)
    left[0].wait_recv()
    cout[5] = (total + cin[4].astype(F32)).astype(BF16)
    left[1].start()
    for head in (4, 28):
        members(head)
    total = quad(8)
    right[1].wait_recv()
    cout[2] = (total + cin[1].astype(F32)).astype(BF16)
    right[2].start()
    total = quad(28)
    left[1].wait_recv()
    cout[6] = (total + cin[5].astype(F32)).astype(BF16)
    left[2].start()
    members(0)
    total = quad(4)
    right[2].wait_recv()
    cout[3] = (total + cin[2].astype(F32)).astype(BF16)
    right[3].start()
    total = quad(0)
    left[2].wait_recv()
    total += cin[6].astype(F32)
    right[3].wait_recv()
    total += cin[3].astype(F32)
    owned = total.astype(BF16)

    urow = iota((8 * CB, 16), 0)
    ucol = iota((8 * CB, 16), 1)
    ublk, uj = urow // 8, lax.rem(urow, 8) - 3
    unpack = one_hot((ucol == uj * CB + ublk) & (uj >= 0) & (uj < 3))
    wide_rows = dot(unpack, owned)
    fresh = jnp.concatenate([wide_rows[cb * 8 : (cb + 1) * 8] for cb in range(CB)], axis=1)
    span = fresh[:, :2304] + context
    gate = pltpu.roll(fresh[:, 2304:4352], 5, 0)

    conv = span * taps[0:1]
    for k in range(1, 4):
        conv += pltpu.roll(span, 8 - k, 0) * taps[k : k + 1]
    live = iota(conv.shape, 0) < 3
    act = jnp.where(live, silu(conv), 0.0)
    x = act[:, :2048]
    inject = act[:, 2048:2176]
    readout = act[:, 2176:2304]
    x1 = pltpu.roll(x, 1, 0)
    x2 = pltpu.roll(x, 2, 0)
    i1 = pltpu.roll(inject, 1, 0)
    i2 = pltpu.roll(inject, 2, 0)

    outs = []
    for g in range(2):
        at_g = slice(g * 1024, (g + 1) * 1024)
        half = slice(g * 64, (g + 1) * 64)
        rd = readout[:, half]
        r_hi = rd.astype(BF16)
        r_lo = (rd - r_hi.astype(F32)).astype(BF16)
        both = jnp.concatenate([r_hi, r_hi], axis=1)
        low = jnp.concatenate([r_lo, jnp.zeros_like(r_lo)], axis=1)
        s_part = s0cat[at_g, :]
        first = dot_nt(both, s_part) + dot_nt(low, s_part)
        d0 = jnp.sum(rd * inject[:, half], axis=1, keepdims=True)
        d1 = jnp.sum(rd * i1[:, half], axis=1, keepdims=True)
        d2 = jnp.sum(rd * i2[:, half], axis=1, keepdims=True)
        response = (
            carry_w[:, at_g] * first
            + mix0[:, at_g] * x[:, at_g] * d0
            + mix1[:, at_g] * x1[:, at_g] * d1
            + mix2[:, at_g] * x2[:, at_g] * d2
            + direct[:, at_g] * x[:, at_g]
        )
        gated = jnp.where(live[:, :1024], response * silu(gate[:, at_g]), 0.0)
        norm = lax.rsqrt(jnp.sum(gated * gated, axis=1, keepdims=True) * (1.0 / 1024) + EPS)
        outs.append(gated * norm * gns[:, at_g])
    gated = jnp.concatenate(outs, axis=1)

    stack = jnp.concatenate([gated[:, cb * GBLK : (cb + 1) * GBLK] for cb in range(CB)], axis=0).astype(BF16)
    prow = iota((16, 8 * CB), 0)
    pcol = iota((16, 8 * CB), 1)
    packed = dot(one_hot(prow == lax.rem(pcol, 8) * CB + pcol // 8), stack)
    rest = gated[:, CB * GBLK :]
    last = jnp.concatenate([rest[j : j + 1] for j in range(3)], axis=1)
    packed = jnp.where(iota((16, GBLK), 0) == 15, jnp.broadcast_to(last, (16, GBLK)), packed)
    gown[...] = packed.astype(BF16)
    gath[z] = packed.astype(BF16)

    def share(src_ref, slot, hop, recv):
        pltpu.make_async_remote_copy(
            src_ref=src_ref, dst_ref=gath.at[slot], send_sem=gsend, recv_sem=recv, device_id={"z": at(hop)},
            device_id_type=MESH,
        ).start()

    for k in (4, 3, 5, 2, 6, 1, 7):
        share(gown, z, 4 * k, grecv.at[k])
    for hop in (-2, -1, 1, 2):
        share(gown, z, hop, nrecv)

    for g in range(2):
        at_g = slice(g * 1024, (g + 1) * 1024)
        half = slice(g * 64, (g + 1) * 64)
        b8 = inject[:, half]
        b_hi = b8.astype(BF16).astype(F32)
        b_lo = b8 - b_hi
        rhs = jnp.concatenate([b_hi, b_lo, b_hi], axis=0).astype(BF16)
        live0 = iota((8, 1024), 0)
        for j in range(3):
            coef = jnp.zeros((8, 1024), F32)
            for i in range(j + 1):
                mix = (mix0, mix1, mix2)[j - i]
                coef = jnp.where(live0 == i, mix[j : j + 1, at_g], coef)
            a8 = coef * x[:, at_g]
            a_hi = a8.astype(BF16).astype(F32)
            a_lo = a8 - a_hi
            lhs = jnp.concatenate([a_hi, a_hi, a_lo], axis=0).astype(BF16)
            snew[j, at_g, :] += dot_tn(lhs, rhs)
    span_v[...] = span.astype(BF16)
    stores = [
        pltpu.make_async_copy(snew, states_o, osem.at[0]),
        pltpu.make_async_copy(span_v, tail_o, osem.at[1]),
    ]
    for cp in stores:
        cp.start()

    for k in (1, 7, 2, 6, 3, 5, 4):
        slot = at(-4 * k)
        pltpu.make_async_remote_copy(
            src_ref=gown, dst_ref=gath.at[slot], send_sem=gsend, recv_sem=grecv.at[k], device_id=partner, device_id_type=MESH
        ).wait_recv()
        for hop in (-1, 1) + ((2,) if k < 4 else (-2,) if k > 4 else ()):
            share(gath.at[slot], slot, hop, nrecv)
    pltpu.make_async_remote_copy(
        src_ref=gath.at[0:24], dst_ref=gath.at[0:24], send_sem=gsend, recv_sem=nrecv, device_id=partner, device_id_type=MESH
    ).wait_recv()

    srow = iota((32 * CB, 128), 0)
    scol = iota((32 * CB, 128), 1)
    m, scb = lax.rem(srow, 32), srow // 32
    select = one_hot((m // 4 == scol // 16) & (lax.rem(scol, 16) == lax.rem(m, 4) * CB + scb) & (lax.rem(m, 4) < 3))
    m2 = iota((32, 128), 0)
    c2 = iota((32, 128), 1)
    pick = [one_hot((m2 // 4 == c2 // 16) & (lax.rem(c2, 16) == 15) & (lax.rem(m2, 4) == j)) for j in range(3)]
    inputs = []
    for tb in range(4):
        block = gath[tb * 8 : (tb + 1) * 8].reshape(128, GBLK)
        y = dot(select, block)
        tail = sum(dot(pick[j], block[:, j * 128 : (j + 1) * 128]) for j in range(3))
        inputs.append(jnp.concatenate([y[cb * 32 : (cb + 1) * 32] for cb in range(CB)] + [tail], axis=1).astype(BF16))
    full = jnp.concatenate(inputs, axis=0)
    own_cols = dot(full, wo[...]).astype(BF16)
    partner_cols = dot(full, wop[...]).astype(BF16)
    for tb in range(4):
        fst[0, tb] = own_cols[tb * 32 : (tb + 1) * 32]
        fst[1, tb] = partner_cols[tb * 32 : (tb + 1) * 32]

    finals = []
    for i, (dc, dt) in enumerate(others):
        to = lax.rem(t + dt, n_tp)
        finals.append(
            pltpu.make_async_remote_copy(
                src_ref=fst.at[dc, to], dst_ref=fin.at[c, t], send_sem=fsend.at[i], recv_sem=frecv.at[i],
                device_id={"c": lax.rem(c + dc, 2), "tp": to}, device_id_type=MESH,
            )
        )
    for cp in finals:
        cp.start()
    fin[c, t] = fst[0, t]
    for cp in finals:
        cp.wait_recv()
    for k in range(2):
        total = fin[k, 0].astype(F32)
        for i in range(1, 4):
            total += fin[k, i].astype(F32)
        mixed_o[k] = total.astype(BF16)

    for cp in stores:
        cp.wait()
    for cp in shares:
        cp.wait_send()
    for cp in right + left:
        cp.wait_send()
    for cp in finals:
        cp.wait_send()
    for ref, count, sem in ((xs, NZ - 1, asend), (part, 24, msend), (gath, NZ - 1, gsend)):
        pltpu.make_async_remote_copy(
            src_ref=ref.at[0:count], dst_ref=ref.at[0:count], send_sem=sem, recv_sem=arecv, device_id=partner,
            device_id_type=MESH,
        ).wait_send()


def local(
    tokens,
    input_norm_scale,
    head_input_matrix,
    output_gate_matrix,
    group_input_matrix,
    group_readout_matrix,
    step_size_matrix,
    step_size_bias,
    log_decay_rate,
    direct_path_weight,
    convolution_tap_weight,
    convolution_history_rows,
    per_proposal_states,
    accepted,
    proposal_extra_decay,
    group_norm_scale,
    output_projection_matrix,
):
    width = tokens.shape[2]
    heads = step_size_bias.shape[0]
    channels = heads * 64
    dma = pltpu.SemaphoreType.DMA
    any_space = pl.BlockSpec(memory_space=pl.ANY)
    smem = pl.BlockSpec(memory_space=pltpu.SMEM)
    vmem = pl.BlockSpec(memory_space=pltpu.VMEM)
    mixed, states, tail = pl.pallas_call(
        kernel,
        name="mixer",
        out_shape=(
            jax.ShapeDtypeStruct((2, 32, 64), BF16),
            jax.ShapeDtypeStruct((3, channels, 64), F32),
            jax.ShapeDtypeStruct((8, 2304), BF16),
        ),
        in_specs=[any_space] * 13 + [smem] + [any_space] * 3,
        out_specs=(vmem, any_space, any_space),
        scratch_shapes=[
            pltpu.VMEM((3, width), BF16),
            pltpu.VMEM((1, width), F32),
            pltpu.VMEM((width, heads), BF16),
            pltpu.VMEM((1, heads), F32),
            pltpu.VMEM((1, heads), F32),
            pltpu.VMEM((1, heads), F32),
            pltpu.VMEM((4, 2, 1152), BF16),
            pltpu.VMEM((6, 2, 1152), BF16),
            pltpu.VMEM((3, channels, 64), F32),
            pltpu.VMEM((3, heads), F32),
            pltpu.VMEM((1, channels), F32),
            pltpu.VMEM((channels, 64), BF16),
            pltpu.VMEM((channels, 64), BF16),
            pltpu.VMEM((CB * 128, BLK), BF16),
            pltpu.VMEM((NZ, 16, 128), BF16),
            pltpu.VMEM((NZ, 16, 128), BF16),
            pltpu.VMEM((NZ, 16, BLK), BF16),
            pltpu.VMEM((8, 4, 16, BLK), BF16),
            pltpu.VMEM((7, 16, BLK), BF16),
            pltpu.VMEM((7, 16, BLK), BF16),
            pltpu.VMEM((NZ, 16, GBLK), BF16),
            pltpu.VMEM((16, GBLK), BF16),
            pltpu.VMEM((2, 4, 32, 64), BF16),
            pltpu.VMEM((2, 4, 32, 64), BF16),
            pltpu.VMEM((3, channels, 64), F32),
            pltpu.VMEM((channels, 128), BF16),
            pltpu.VMEM((8, 2304), BF16),
            dma((12 + len(PIECES),)),
            dma((len(PIECES) + 1,)),
            dma((len(PIECES) + 1,)),
            dma,
            dma,
            dma,
            dma((8,)),
            dma((7,)),
            dma((7,)),
            dma,
            dma((8,)),
            dma,
            dma((7,)),
            dma((7,)),
            dma((2,)),
        ],
        compiler_params=pltpu.CompilerParams(
            collective_id=0, has_side_effects=True, vmem_limit_bytes=56 * 1024 * 1024
        ),
    )(
        tokens,
        input_norm_scale.reshape(1, width),
        head_input_matrix,
        output_gate_matrix,
        group_input_matrix,
        group_readout_matrix,
        step_size_matrix,
        step_size_bias.reshape(1, heads),
        log_decay_rate.reshape(1, heads),
        direct_path_weight.reshape(1, heads),
        convolution_tap_weight,
        convolution_history_rows,
        per_proposal_states.reshape(3, channels, 64),
        accepted,
        proposal_extra_decay,
        group_norm_scale.reshape(1, channels),
        output_projection_matrix,
    )
    mixed = mixed.reshape(2, 8, 4, 64)[:, :, :3].transpose(1, 0, 2, 3).reshape(16, 3, 64)
    states = states.reshape(1, 3, heads, 64, 64)
    rows = tail[:6]
    groups = [
        jnp.concatenate(
            [
                rows[:, g * 1024 : (g + 1) * 1024],
                rows[:, 2048 + g * 64 : 2048 + (g + 1) * 64],
                rows[:, 2176 + g * 64 : 2176 + (g + 1) * 64],
            ],
            axis=1,
        )
        for g in range(2)
    ]
    tail = jnp.stack(groups, axis=1)[None]
    return mixed, states, tail


def solution(mesh):
    ring = mesh.shape["kv"] // 2
    assert ring == NZ and mesh.shape["tp"] == 4
    finer = Mesh(
        mesh.devices.reshape(mesh.shape["grp"], ring, 2, mesh.shape["tp"]),
        ("grp", "z", "c", "tp"),
    )
    return jax.shard_map(
        local,
        mesh=finer,
        in_specs=(
            P(GRP_KV, None, None),
            P(),
            P(KV, "tp"),
            P(KV, "tp"),
            P(KV, "tp"),
            P(KV, "tp"),
            P(None, "tp"),
            P("tp"),
            P("tp"),
            P("tp"),
            P(None, "tp", None),
            P(GRP_KV, None, "tp", None),
            P(GRP_KV, None, "tp", None, None),
            P(GRP_KV),
            P(GRP_KV, None, "tp"),
            P("tp"),
            P("tp", KV),
        ),
        out_specs=(
            P(("grp", "tp"), None, KV),
            P(GRP_KV, None, "tp", None, None),
            P(GRP_KV, None, "tp", None),
        ),
        check_vma=False,
    )
```

```python
import functools

import jax
import jax.numpy as jnp
from jax import lax
from jax.experimental import pallas as pl
from jax.experimental.pallas import tpu as pltpu
from jax.sharding import Mesh
from jax.sharding import PartitionSpec as P

MESH = pl.DeviceIdType.MESH
EPS = 1e-06
F32 = jnp.float32
BF16 = jnp.bfloat16

KV = ("z", "c")
GRP_KV = ("grp", "z", "c")

NZ = 32
BLK = 896
CB = 5
GBLK = 384


def iota(shape, dim):
    return lax.broadcasted_iota(jnp.int32, shape, dim)


def split3(v):
    hi = v.astype(BF16)
    rest = v - hi.astype(F32)
    mid = rest.astype(BF16)
    lo = (rest - mid.astype(F32)).astype(BF16)
    return hi, mid, lo


def dot(a, b):
    return jnp.dot(a, b, preferred_element_type=F32)


def dot_nt(a, b):
    return lax.dot_general(a, b, (((1,), (1,)), ((), ())), preferred_element_type=F32)


def dot_tn(a, b):
    return lax.dot_general(a, b, (((0,), (0,)), ((), ())), preferred_element_type=F32)


def silu(v):
    return v / (1.0 + jnp.exp(-v))


def one_hot(cond):
    return jnp.where(cond, 1.0, 0.0).astype(BF16)


PIECES = (
    (0, 0, 896, 0, 0),
    (0, 896, 896, 1, 0),
    (0, 1792, 256, 2, 0),
    (2, 0, 128, 2, 256),
    (3, 0, 128, 2, 384),
    (1, 0, 384, 2, 512),
    (1, 384, 896, 3, 0),
    (1, 1280, 768, 4, 0),
)


def kernel(
    tok_h, ins_h, wh_h, wg_h, wi_h, wr_h, ws_h, bias_h, ldr_h, dpw_h, tap_h, hist_h, st_h, acc_s, ped_h, gns_h, wo_h,
    mixed_o, snew, tail_o,
    tok, ins, ws, bias, ldr, dpw, tap, hist, st, ped, gns, wo, wop,
    w2, nst, xs, part, mem, cout, cin, gath, gown, fin, fst, s0cat,
    lsem, wsend, wrecv, asend, arecv, msend, mrecv, csend, crecv, gsend, grecv, nrecv, fsend, frecv,
):
    z = lax.axis_index("z")
    c = lax.axis_index("c")
    t = lax.axis_index("tp")
    n_tp = lax.axis_size("tp")

    def at(offset):
        return lax.rem(z + (offset + NZ) % NZ, NZ)

    barrier = pltpu.get_barrier_semaphore()

    def greet(k, _):
        pl.semaphore_signal(barrier, inc=1, device_id={"z": lax.rem(z + k, NZ)}, device_id_type=MESH)
        return 0

    lax.fori_loop(1, NZ, greet, 0)
    others = [(dc, dt) for dc in range(2) for dt in range(n_tp) if (dc, dt) != (0, 0)]
    for dc, dt in others:
        pl.semaphore_signal(
            barrier, inc=1, device_id={"c": lax.rem(c + dc, 2), "tp": lax.rem(t + dt, n_tp)}, device_id_type=MESH
        )

    pairs = [
        (tok_h.at[0], tok), (ins_h, ins), (ws_h, ws), (bias_h, bias), (ldr_h, ldr), (dpw_h, dpw), (tap_h, tap),
        (hist_h.at[0], hist), (ped_h, ped), (gns_h, gns), (st_h, st), (wo_h, wo),
    ]
    loads = [pltpu.make_async_copy(src, dst, lsem.at[i]) for i, (src, dst) in enumerate(pairs)]
    sources = (wh_h, wg_h, wi_h, wr_h)
    mine = pl.multiple_of(c * 64, 64)
    for i, (source, first, count, row, lane) in enumerate(PIECES):
        loads.append(
            pltpu.make_async_copy(
                sources[source].at[:, first : first + count],
                w2.at[pl.ds(pl.multiple_of(row * 128 + mine, 64), 64), lane : lane + count],
                lsem.at[len(pairs) + i],
            )
        )
    for cp in loads:
        cp.start()

    loads[0].wait()
    loads[1].wait()
    wide = tok[...].astype(F32)
    scale = lax.rsqrt(jnp.sum(wide * wide, axis=-1, keepdims=True) * (1.0 / wide.shape[1]) + EPS)
    normed = (wide * scale * ins[...]).astype(BF16)
    row16 = iota((16, 3), 0)
    spread = one_hot((row16 // CB == iota((16, 3), 1)) & (row16 < 3 * CB))
    sent = dot(spread, normed).astype(BF16)
    for k in range(NZ):
        nst[k] = sent[:, k * 128 : (k + 1) * 128]

    pl.semaphore_wait(barrier, NZ - 1 + len(others))

    def send_slice(k, _):
        to = lax.rem(z + k, NZ)
        pltpu.make_async_remote_copy(
            src_ref=nst.at[to], dst_ref=xs.at[z], send_sem=asend, recv_sem=arecv, device_id={"z": to}, device_id_type=MESH
        ).start()
        return 0

    lax.fori_loop(1, NZ, send_slice, 0)
    xs[z] = nst[z]

    partner = {"c": 1 - c}
    shares = []
    for i, (source, first, count, row, lane) in enumerate(PIECES):
        shares.append(
            pltpu.make_async_remote_copy(
                src_ref=sources[source].at[:, first : first + count],
                dst_ref=w2.at[pl.ds(pl.multiple_of(row * 128 + mine, 64), 64), lane : lane + count],
                send_sem=wsend.at[i], recv_sem=wrecv.at[i], device_id=partner, device_id_type=MESH,
            )
        )
    shares.append(
        pltpu.make_async_remote_copy(
            src_ref=wo_h, dst_ref=wop, send_sem=wsend.at[len(PIECES)], recv_sem=wrecv.at[len(PIECES)],
            device_id=partner, device_id_type=MESH,
        )
    )
    for cp in shares:
        cp.start()

    for cp in loads[2:]:
        cp.wait()
    w2[4 * 128 :, 768:] = jnp.zeros((128, 128), BF16)
    step_raw = dot_nt(normed, ws[...])
    raw = step_raw + bias[...]
    step = jnp.maximum(raw, 0.0) + jnp.log1p(jnp.exp(-jnp.abs(raw)))
    decay = jnp.exp(ldr[...]) * step
    cum0 = ped[0] - decay[0:1]
    cum1 = cum0 + (ped[1] - decay[1:2])
    cum2 = cum1 + (ped[2] - decay[2:3])
    none = jnp.zeros_like(cum0)
    zeros5 = jnp.zeros((5, cum0.shape[1]), F32)

    def rows(a, b, d):
        return jnp.concatenate([a, b, d, zeros5], axis=0)

    per_head = jnp.concatenate(
        [
            rows(jnp.exp(cum0), jnp.exp(cum1), jnp.exp(cum2)),
            rows(step[0:1], step[1:2], step[2:3]),
            rows(none, jnp.exp(cum1 - cum0) * step[0:1], jnp.exp(cum2 - cum1) * step[1:2]),
            rows(none, none, jnp.exp(cum2 - cum0) * step[0:1]),
            rows(dpw[...], dpw[...], dpw[...]),
        ],
        axis=0,
    )
    heads = per_head.shape[1]
    lanes = heads * 64
    to_head = iota((heads, lanes), 1) - iota((heads, lanes), 0) * 64
    expand = one_hot((to_head >= 0) & (to_head < 64))
    hi, mid, lo = split3(per_head)
    wide_heads = dot(hi, expand) + dot(mid, expand) + dot(lo, expand)
    carry_w, mix0, mix1, mix2, direct = (wide_heads[i * 8 : (i + 1) * 8] for i in range(5))

    start = jnp.clip(acc_s[0] - 1, 0, 2)
    ones3 = jnp.ones((3, 64), BF16)
    for g in range(2):
        at_g = slice(g * 1024, (g + 1) * 1024)
        s0 = st[start, at_g, :]
        s_hi = s0.astype(BF16)
        s_lo = (s0 - s_hi.astype(F32)).astype(BF16)
        s0cat[at_g, :] = jnp.concatenate([s_hi, s_lo], axis=1)
        for j in range(3):
            line = carry_w[j : j + 1, at_g]
            l_hi, l_mid, l_lo = split3(line)
            stack = jnp.concatenate([l_hi.astype(F32), l_mid.astype(F32), l_lo.astype(F32)], axis=0).astype(BF16)
            snew[j, at_g, :] = dot_tn(stack, ones3) * s0

    def in_order(v):
        a, b = v[:, 0, :], v[:, 1, :]
        return jnp.concatenate(
            [a[:, :1024], b[:, :1024], a[:, 1024:1088], b[:, 1024:1088], a[:, 1088:], b[:, 1088:]], axis=1
        )

    kept = in_order(hist[...].astype(F32))
    taps = in_order(tap[...].astype(F32))
    accepted = acc_s[0]
    context = jnp.where(accepted == 1, kept[1:4], jnp.where(accepted == 2, kept[2:5], kept[3:6]))
    context = jnp.concatenate([context, jnp.zeros((5, context.shape[1]), F32)], axis=0)

    for cp in shares:
        cp.wait_recv()
    pltpu.make_async_remote_copy(
        src_ref=nst.at[0 : NZ - 1], dst_ref=xs.at[0 : NZ - 1], send_sem=asend, recv_sem=arecv, device_id=partner,
        device_id_type=MESH,
    ).wait_recv()
    x_all = xs[...].reshape(NZ * 16, 128)
    block_of = lax.rem(lax.rem(iota((NZ * 16, 128), 0), 16), CB)
    zero = jnp.zeros_like(x_all)
    stacked = jnp.concatenate([jnp.where(block_of == cb, x_all, zero) for cb in range(CB)], axis=1)
    for n0, n1 in ((0, 256), (256, 512), (512, 768), (768, 896)):
        part[:, :, n0:n1] = dot(stacked, w2[:, n0:n1]).astype(BF16).reshape(NZ, 16, n1 - n0)

    def member(delta, hop, head, slot):
        pltpu.make_async_remote_copy(
            src_ref=part.at[at(delta)], dst_ref=mem.at[head // 4, slot], send_sem=msend, recv_sem=mrecv.at[head // 4],
            device_id={"z": at(hop)}, device_id_type=MESH,
        ).start()

    def members(head):
        member((head + 1) % NZ, 1, head, 0)
        member((head - 1) % NZ, -1, head, 1)
        if head < 16:
            member(head + 2, 2, head, 2)
        if head > 16:
            member(head - 2, -2, head, 2)
        if head == 0:
            member(NZ - 2, -2, head, 3)

    def quad(head):
        count = {0: 4, 16: 2}.get(head, 3)
        pltpu.make_async_remote_copy(
            src_ref=mem.at[head // 4, 0:count], dst_ref=mem.at[head // 4, 0:count], send_sem=msend,
            recv_sem=mrecv.at[head // 4], device_id=partner, device_id_type=MESH,
        ).wait_recv()
        total = part[at(head)].astype(F32)
        for slot in range(count):
            total += mem[head // 4, slot].astype(F32)
        return total

    def chain(step_at, hop):
        return pltpu.make_async_remote_copy(
            src_ref=cout.at[step_at], dst_ref=cin.at[step_at], send_sem=csend.at[step_at], recv_sem=crecv.at[step_at],
            device_id={"z": at(hop)}, device_id_type=MESH,
        )

    right = [chain(i, 4) for i in range(4)]
    left = [chain(4 + i, -4) for i in range(3)]
    for head in (16, 12, 20):
        members(head)
    cout[0] = quad(16).astype(BF16)
    right[0].start()
    cout[4] = quad(20).astype(BF16)
    left[0].start()
    for head in (8, 24):
        members(head)
    total = quad(12)
    right[0].wait_recv()
    cout[1] = (total + cin[0].astype(F32)).astype(BF16)
    right[1].start()
    total = quad(24)
    left[0].wait_recv()
    cout[5] = (total + cin[4].astype(F32)).astype(BF16)
    left[1].start()
    for head in (4, 28):
        members(head)
    total = quad(8)
    right[1].wait_recv()
    cout[2] = (total + cin[1].astype(F32)).astype(BF16)
    right[2].start()
    total = quad(28)
    left[1].wait_recv()
    cout[6] = (total + cin[5].astype(F32)).astype(BF16)
    left[2].start()
    members(0)
    total = quad(4)
    right[2].wait_recv()
    cout[3] = (total + cin[2].astype(F32)).astype(BF16)
    right[3].start()
    total = quad(0)
    left[2].wait_recv()
    total += cin[6].astype(F32)
    right[3].wait_recv()
    total += cin[3].astype(F32)
    owned = total.astype(BF16)

    urow = iota((8 * CB, 16), 0)
    ucol = iota((8 * CB, 16), 1)
    ublk, uj = urow // 8, lax.rem(urow, 8) - 3
    unpack = one_hot((ucol == uj * CB + ublk) & (uj >= 0) & (uj < 3))
    wide_rows = dot(unpack, owned)
    fresh = jnp.concatenate([wide_rows[cb * 8 : (cb + 1) * 8] for cb in range(CB)], axis=1)
    span = fresh[:, :2304] + context
    gate = pltpu.roll(fresh[:, 2304:4352], 5, 0)

    conv = span * taps[0:1]
    for k in range(1, 4):
        conv += pltpu.roll(span, 8 - k, 0) * taps[k : k + 1]
    live = iota(conv.shape, 0) < 3
    act = jnp.where(live, silu(conv), 0.0)
    x = act[:, :2048]
    inject = act[:, 2048:2176]
    readout = act[:, 2176:2304]
    x1 = pltpu.roll(x, 1, 0)
    x2 = pltpu.roll(x, 2, 0)
    i1 = pltpu.roll(inject, 1, 0)
    i2 = pltpu.roll(inject, 2, 0)

    outs = []
    for g in range(2):
        at_g = slice(g * 1024, (g + 1) * 1024)
        half = slice(g * 64, (g + 1) * 64)
        rd = readout[:, half]
        r_hi = rd.astype(BF16)
        r_lo = (rd - r_hi.astype(F32)).astype(BF16)
        both = jnp.concatenate([r_hi, r_hi], axis=1)
        low = jnp.concatenate([r_lo, jnp.zeros_like(r_lo)], axis=1)
        s_part = s0cat[at_g, :]
        first = dot_nt(both, s_part) + dot_nt(low, s_part)
        d0 = jnp.sum(rd * inject[:, half], axis=1, keepdims=True)
        d1 = jnp.sum(rd * i1[:, half], axis=1, keepdims=True)
        d2 = jnp.sum(rd * i2[:, half], axis=1, keepdims=True)
        response = (
            carry_w[:, at_g] * first
            + mix0[:, at_g] * x[:, at_g] * d0
            + mix1[:, at_g] * x1[:, at_g] * d1
            + mix2[:, at_g] * x2[:, at_g] * d2
            + direct[:, at_g] * x[:, at_g]
        )
        gated = jnp.where(live[:, :1024], response * silu(gate[:, at_g]), 0.0)
        norm = lax.rsqrt(jnp.sum(gated * gated, axis=1, keepdims=True) * (1.0 / 1024) + EPS)
        outs.append(gated * norm * gns[:, at_g])
    gated = jnp.concatenate(outs, axis=1)

    stack = jnp.concatenate([gated[:, cb * GBLK : (cb + 1) * GBLK] for cb in range(CB)], axis=0).astype(BF16)
    prow = iota((16, 8 * CB), 0)
    pcol = iota((16, 8 * CB), 1)
    packed = dot(one_hot(prow == lax.rem(pcol, 8) * CB + pcol // 8), stack)
    rest = gated[:, CB * GBLK :]
    last = jnp.concatenate([rest[j : j + 1] for j in range(3)], axis=1)
    packed = jnp.where(iota((16, GBLK), 0) == 15, jnp.broadcast_to(last, (16, GBLK)), packed)
    gown[...] = packed.astype(BF16)
    gath[z] = packed.astype(BF16)

    def share(src_ref, slot, hop, recv):
        pltpu.make_async_remote_copy(
            src_ref=src_ref, dst_ref=gath.at[slot], send_sem=gsend, recv_sem=recv, device_id={"z": at(hop)},
            device_id_type=MESH,
        ).start()

    for k in (4, 3, 5, 2, 6, 1, 7):
        share(gown, z, 4 * k, grecv.at[k])
    for hop in (-2, -1, 1, 2):
        share(gown, z, hop, nrecv)

    for g in range(2):
        at_g = slice(g * 1024, (g + 1) * 1024)
        half = slice(g * 64, (g + 1) * 64)
        b8 = inject[:, half]
        b_hi = b8.astype(BF16).astype(F32)
        b_lo = b8 - b_hi
        rhs = jnp.concatenate([b_hi, b_lo, b_hi], axis=0).astype(BF16)
        live0 = iota((8, 1024), 0)
        for j in range(3):
            coef = jnp.zeros((8, 1024), F32)
            for i in range(j + 1):
                mix = (mix0, mix1, mix2)[j - i]
                coef = jnp.where(live0 == i, mix[j : j + 1, at_g], coef)
            a8 = coef * x[:, at_g]
            a_hi = a8.astype(BF16).astype(F32)
            a_lo = a8 - a_hi
            lhs = jnp.concatenate([a_hi, a_hi, a_lo], axis=0).astype(BF16)
            snew[j, at_g, :] += dot_tn(lhs, rhs)
    groups = [
        jnp.concatenate(
            [
                span[:, g * 1024 : (g + 1) * 1024],
                span[:, 2048 + g * 64 : 2048 + (g + 1) * 64],
                span[:, 2176 + g * 64 : 2176 + (g + 1) * 64],
            ],
            axis=1,
        )
        for g in range(2)
    ]
    for i in range(6):
        tail_o[i] = jnp.concatenate([groups[0][i : i + 1], groups[1][i : i + 1]], axis=0).astype(BF16)

    for k in (1, 7, 2, 6, 3, 5, 4):
        slot = at(-4 * k)
        pltpu.make_async_remote_copy(
            src_ref=gown, dst_ref=gath.at[slot], send_sem=gsend, recv_sem=grecv.at[k], device_id=partner, device_id_type=MESH
        ).wait_recv()
        for hop in (-1, 1) + ((2,) if k < 4 else (-2,) if k > 4 else ()):
            share(gath.at[slot], slot, hop, nrecv)
    pltpu.make_async_remote_copy(
        src_ref=gath.at[0:24], dst_ref=gath.at[0:24], send_sem=gsend, recv_sem=nrecv, device_id=partner, device_id_type=MESH
    ).wait_recv()

    srow = iota((32 * CB, 128), 0)
    scol = iota((32 * CB, 128), 1)
    m, scb = lax.rem(srow, 32), srow // 32
    select = one_hot((m // 4 == scol // 16) & (lax.rem(scol, 16) == lax.rem(m, 4) * CB + scb) & (lax.rem(m, 4) < 3))
    m2 = iota((32, 128), 0)
    c2 = iota((32, 128), 1)
    pick = [one_hot((m2 // 4 == c2 // 16) & (lax.rem(c2, 16) == 15) & (lax.rem(m2, 4) == j)) for j in range(3)]
    inputs = []
    for tb in range(4):
        block = gath[tb * 8 : (tb + 1) * 8].reshape(128, GBLK)
        y = dot(select, block)
        tail = sum(dot(pick[j], block[:, j * 128 : (j + 1) * 128]) for j in range(3))
        inputs.append(jnp.concatenate([y[cb * 32 : (cb + 1) * 32] for cb in range(CB)] + [tail], axis=1).astype(BF16))
    full = jnp.concatenate(inputs, axis=0)
    own_cols = dot_nt(full, wo[...]).astype(BF16)
    partner_cols = dot_nt(full, wop[...]).astype(BF16)
    for tb in range(4):
        fst[0, tb] = own_cols[tb * 32 : (tb + 1) * 32]
        fst[1, tb] = partner_cols[tb * 32 : (tb + 1) * 32]

    finals = []
    for i, (dc, dt) in enumerate(others):
        to = lax.rem(t + dt, n_tp)
        finals.append(
            pltpu.make_async_remote_copy(
                src_ref=fst.at[dc, to], dst_ref=fin.at[c, t], send_sem=fsend.at[i], recv_sem=frecv.at[i],
                device_id={"c": lax.rem(c + dc, 2), "tp": to}, device_id_type=MESH,
            )
        )
    for cp in finals:
        cp.start()
    fin[c, t] = fst[0, t]
    for cp in finals:
        cp.wait_recv()
    totals = []
    for k in range(2):
        total = fin[k, 0].astype(F32)
        for i in range(1, 4):
            total += fin[k, i].astype(F32)
        totals.append(total.astype(BF16))
    trow = iota((48, 32), 0)
    tcol = iota((48, 32), 1)
    want = 4 * (lax.rem(trow, 16) // 2) + trow // 16
    arranged = sum(dot(one_hot((lax.rem(trow, 2) == k) & (tcol == want)), totals[k]) for k in range(2))
    for j in range(3):
        mixed_o[j] = arranged[j * 16 : (j + 1) * 16].astype(BF16)

    for cp in shares:
        cp.wait_send()
    for cp in right + left:
        cp.wait_send()
    for cp in finals:
        cp.wait_send()
    for ref, count, sem in ((xs, NZ - 1, asend), (part, 24, msend), (gath, NZ - 1, gsend)):
        pltpu.make_async_remote_copy(
            src_ref=ref.at[0:count], dst_ref=ref.at[0:count], send_sem=sem, recv_sem=arecv, device_id=partner,
            device_id_type=MESH,
        ).wait_send()


def store(mixed, states, tail, mixed_o, states_o, tail_o, sem):
    copies = [
        pltpu.make_async_copy(src, dst, sem.at[i])
        for i, (src, dst) in enumerate(((states, states_o), (tail, tail_o), (mixed, mixed_o)))
    ]
    for cp in copies:
        cp.start()
    for cp in copies:
        cp.wait()


def local(
    tokens,
    input_norm_scale,
    head_input_matrix,
    output_gate_matrix,
    group_input_matrix,
    group_readout_matrix,
    step_size_matrix,
    step_size_bias,
    log_decay_rate,
    direct_path_weight,
    convolution_tap_weight,
    convolution_history_rows,
    per_proposal_states,
    accepted,
    proposal_extra_decay,
    group_norm_scale,
    output_projection_matrix,
):
    width = tokens.shape[2]
    heads = step_size_bias.shape[0]
    channels = heads * 64
    dma = pltpu.SemaphoreType.DMA
    any_space = pl.BlockSpec(memory_space=pl.ANY)
    smem = pl.BlockSpec(memory_space=pltpu.SMEM)
    vmem = pl.BlockSpec(memory_space=pltpu.VMEM)
    mixed, states, tail = pl.pallas_call(
        kernel,
        name="mixer",
        out_shape=(
            pltpu.VMEM((3, 16, 64), BF16),
            pltpu.VMEM((3, channels, 64), F32),
            pltpu.VMEM((6, 2, 1152), BF16),
        ),
        in_specs=[any_space] * 13 + [smem] + [any_space] * 3,
        out_specs=(vmem, vmem, vmem),
        scratch_shapes=[
            pltpu.VMEM((3, width), BF16),
            pltpu.VMEM((1, width), F32),
            pltpu.VMEM((heads, width), BF16),
            pltpu.VMEM((1, heads), F32),
            pltpu.VMEM((1, heads), F32),
            pltpu.VMEM((1, heads), F32),
            pltpu.VMEM((4, 2, 1152), BF16),
            pltpu.VMEM((6, 2, 1152), BF16),
            pltpu.VMEM((3, channels, 64), F32),
            pltpu.VMEM((3, 1, heads), F32),
            pltpu.VMEM((1, channels), F32),
            pltpu.VMEM((64, channels), BF16),
            pltpu.VMEM((64, channels), BF16),
            pltpu.VMEM((CB * 128, BLK), BF16),
            pltpu.VMEM((NZ, 16, 128), BF16),
            pltpu.VMEM((NZ, 16, 128), BF16),
            pltpu.VMEM((NZ, 16, BLK), BF16),
            pltpu.VMEM((8, 4, 16, BLK), BF16),
            pltpu.VMEM((7, 16, BLK), BF16),
            pltpu.VMEM((7, 16, BLK), BF16),
            pltpu.VMEM((NZ, 16, GBLK), BF16),
            pltpu.VMEM((16, GBLK), BF16),
            pltpu.VMEM((2, 4, 32, 64), BF16),
            pltpu.VMEM((2, 4, 32, 64), BF16),
            pltpu.VMEM((channels, 128), BF16),
            dma((12 + len(PIECES),)),
            dma((len(PIECES) + 1,)),
            dma((len(PIECES) + 1,)),
            dma,
            dma,
            dma,
            dma((8,)),
            dma((7,)),
            dma((7,)),
            dma,
            dma((8,)),
            dma,
            dma((7,)),
            dma((7,)),
        ],
        compiler_params=pltpu.CompilerParams(
            collective_id=0, has_side_effects=True, vmem_limit_bytes=56 * 1024 * 1024
        ),
    )(
        tokens,
        input_norm_scale.reshape(1, width),
        head_input_matrix,
        output_gate_matrix,
        group_input_matrix,
        group_readout_matrix,
        step_size_matrix.T,
        step_size_bias.reshape(1, heads),
        log_decay_rate.reshape(1, heads),
        direct_path_weight.reshape(1, heads),
        convolution_tap_weight,
        convolution_history_rows,
        per_proposal_states.reshape(3, channels, 64),
        accepted,
        proposal_extra_decay.transpose(1, 0, 2),
        group_norm_scale.reshape(1, channels),
        output_projection_matrix.T,
    )
    mixed, states, tail = pl.pallas_call(
        store,
        name="store",
        out_shape=(
            jax.ShapeDtypeStruct((3, 16, 64), BF16),
            jax.ShapeDtypeStruct((3, channels, 64), F32),
            jax.ShapeDtypeStruct((6, 2, 1152), BF16),
        ),
        in_specs=[pl.BlockSpec(memory_space=pltpu.VMEM)] * 3,
        out_specs=(any_space,) * 3,
        scratch_shapes=[dma((3,))],
    )(*(pltpu.with_memory_space_constraint(v, pltpu.VMEM) for v in (mixed, states, tail)))
    mixed = mixed.transpose(1, 0, 2)
    states = states.reshape(1, 3, heads, 64, 64)
    tail = tail[None]
    return mixed, states, tail


def solution(mesh):
    ring = mesh.shape["kv"] // 2
    assert ring == NZ and mesh.shape["tp"] == 4
    finer = Mesh(
        mesh.devices.reshape(mesh.shape["grp"], ring, 2, mesh.shape["tp"]),
        ("grp", "z", "c", "tp"),
    )
    return jax.shard_map(
        local,
        mesh=finer,
        in_specs=(
            P(GRP_KV, None, None),
            P(),
            P(KV, "tp"),
            P(KV, "tp"),
            P(KV, "tp"),
            P(KV, "tp"),
            P(None, "tp"),
            P("tp"),
            P("tp"),
            P("tp"),
            P(None, "tp", None),
            P(GRP_KV, None, "tp", None),
            P(GRP_KV, None, "tp", None, None),
            P(GRP_KV),
            P(GRP_KV, None, "tp"),
            P("tp"),
            P("tp", KV),
        ),
        out_specs=(
            P(("grp", "tp"), None, KV),
            P(GRP_KV, None, "tp", None, None),
            P(GRP_KV, None, "tp", None),
        ),
        check_vma=False,
    )
```

```python
import functools

import jax
import jax.numpy as jnp
from jax import lax
from jax.experimental import pallas as pl
from jax.experimental.pallas import tpu as pltpu
from jax.sharding import Mesh
from jax.sharding import PartitionSpec as P

MESH = pl.DeviceIdType.MESH
EPS = 1e-06
F32 = jnp.float32
BF16 = jnp.bfloat16

KV = ("z", "c")
GRP_KV = ("grp", "z", "c")

NZ = 32
BLK = 896
CB = 5
GBLK = 384


def iota(shape, dim):
    return lax.broadcasted_iota(jnp.int32, shape, dim)


def split3(v):
    hi = v.astype(BF16)
    rest = v - hi.astype(F32)
    mid = rest.astype(BF16)
    lo = (rest - mid.astype(F32)).astype(BF16)
    return hi, mid, lo


def dot(a, b):
    return jnp.dot(a, b, preferred_element_type=F32)


def dot_nt(a, b):
    return lax.dot_general(a, b, (((1,), (1,)), ((), ())), preferred_element_type=F32)


def dot_tn(a, b):
    return lax.dot_general(a, b, (((0,), (0,)), ((), ())), preferred_element_type=F32)


def silu(v):
    return v / (1.0 + jnp.exp(-v))


def one_hot(cond):
    return jnp.where(cond, 1.0, 0.0).astype(BF16)


PIECES = (
    (0, 0, 896, 0, 0),
    (0, 896, 896, 1, 0),
    (0, 1792, 256, 2, 0),
    (2, 0, 128, 2, 256),
    (3, 0, 128, 2, 384),
    (1, 0, 384, 2, 512),
    (1, 384, 896, 3, 0),
    (1, 1280, 768, 4, 0),
)


def kernel(
    tok_h, ins_h, wh_h, wg_h, wi_h, wr_h, ws_h, bias_h, ldr_h, dpw_h, tap_h, hist_h, st_h, acc_s, ped_h, gns_h, wo_h,
    mixed_o, snew, tail_o,
    tok, ins, ws, bias, ldr, dpw, tap, hist, st, ped, gns, wo, wop,
    w2, nst, xs, part, mem, cout, cin, gath, gown, fin, fst, s0cat,
    lsem, wsend, wrecv, asend, arecv, msend, mrecv, csend, crecv, gsend, grecv, nrecv, fsend, frecv, rel0, rel1, r0send, r0recv, r1send, r1recv, may,
):
    z = lax.axis_index("z")
    c = lax.axis_index("c")
    t = lax.axis_index("tp")
    n_tp = lax.axis_size("tp")

    o = lax.rem(z + NZ - 1, NZ)

    def at(offset):
        return lax.rem(z + (offset + NZ) % NZ, NZ)

    def chip(place):
        return lax.rem(place + 1, NZ)

    pairs = [
        (tok_h.at[0], tok), (ins_h, ins), (ws_h, ws), (bias_h, bias), (ldr_h, ldr), (dpw_h, dpw), (tap_h, tap),
        (hist_h.at[0], hist), (ped_h, ped), (gns_h, gns), (st_h, st), (wo_h, wo),
    ]
    loads = [pltpu.make_async_copy(src, dst, lsem.at[i]) for i, (src, dst) in enumerate(pairs)]
    sources = (wh_h, wg_h, wi_h, wr_h)
    mine = pl.multiple_of(c * 64, 64)
    for i, (source, first, count, row, lane) in enumerate(PIECES):
        loads.append(
            pltpu.make_async_copy(
                sources[source].at[:, first : first + count],
                w2.at[pl.ds(pl.multiple_of(row * 128 + mine, 64), 64), lane : lane + count],
                lsem.at[len(pairs) + i],
            )
        )
    for cp in loads:
        cp.start()

    barrier = pltpu.get_barrier_semaphore()

    def greet(to, _):
        pl.semaphore_signal(barrier, inc=1, device_id={"z": chip(to)}, device_id_type=MESH)
        return 0

    lax.fori_loop(o + 1, NZ, greet, 0)
    others = [(dc, dt) for dc in range(2) for dt in range(n_tp) if (dc, dt) != (0, 0)]
    for dc, dt in others:
        pl.semaphore_signal(
            barrier, inc=1, device_id={"c": lax.rem(c + dc, 2), "tp": lax.rem(t + dt, n_tp)}, device_id_type=MESH
        )

    pl.semaphore_wait(barrier, o + len(others))

    def tell(k, _):
        to = chip(o - k)

        @pl.when((k <= 8) | (k >= 24) | ((k >= 17) & (o < 24)))
        def _():
            pl.semaphore_signal(may.at[o], inc=1, device_id={"z": to}, device_id_type=MESH)

        return 0

    lax.fori_loop(1, o + 1, tell, 0)

    loads[0].wait()
    loads[1].wait()
    wide = tok[...].astype(F32)
    scale = lax.rsqrt(jnp.sum(wide * wide, axis=-1, keepdims=True) * (1.0 / wide.shape[1]) + EPS)
    normed = (wide * scale * ins[...]).astype(BF16)
    padded = jnp.concatenate([normed.astype(F32), jnp.zeros((1, normed.shape[1]), F32)], axis=0).astype(BF16)
    for k in range(NZ):
        nst[k] = padded[:, k * 128 : (k + 1) * 128]

    def copy_slice(src_ref, dst_ref, send_sem, recv_sem, to):
        return pltpu.make_async_remote_copy(
            src_ref=src_ref, dst_ref=dst_ref, send_sem=send_sem, recv_sem=recv_sem, device_id={"z": chip(to)},
            device_id_type=MESH,
        )

    def direct_slice(to):
        copy_slice(nst.at[chip(to)], xs.at[z], asend, arecv, to).start()

    def send_back(to, _):
        direct_slice(to)
        return 0

    lax.fori_loop(0, o, send_back, 0)

    def send_by_first(to, _):
        relay = to - 24
        copy_slice(nst.at[chip(to)], rel1.at[o - relay - 1], asend, r1recv.at[o - relay - 1], relay).start()
        return 0

    lax.fori_loop(jnp.maximum(o + 17, 24), jnp.minimum(o + 24, NZ), send_by_first, 0)
    xs[z] = nst[z]

    partner = {"c": 1 - c}
    shares = []
    for i, (source, first, count, row, lane) in enumerate(PIECES):
        shares.append(
            pltpu.make_async_remote_copy(
                src_ref=sources[source].at[:, first : first + count],
                dst_ref=w2.at[pl.ds(pl.multiple_of(row * 128 + mine, 64), 64), lane : lane + count],
                send_sem=wsend.at[i], recv_sem=wrecv.at[i], device_id=partner, device_id_type=MESH,
            )
        )
    shares.append(
        pltpu.make_async_remote_copy(
            src_ref=wo_h, dst_ref=wop, send_sem=wsend.at[len(PIECES)], recv_sem=wrecv.at[len(PIECES)],
            device_id=partner, device_id_type=MESH,
        )
    )
    for cp in shares:
        cp.start()

    for cp in loads[2:]:
        cp.wait()
    w2[4 * 128 :, 768:] = jnp.zeros((128, 128), BF16)
    step_raw = dot_nt(normed, ws[...])
    raw = step_raw + bias[...]
    step = jnp.maximum(raw, 0.0) + jnp.log1p(jnp.exp(-jnp.abs(raw)))
    decay = jnp.exp(ldr[...]) * step
    cum0 = ped[0] - decay[0:1]
    cum1 = cum0 + (ped[1] - decay[1:2])
    cum2 = cum1 + (ped[2] - decay[2:3])
    none = jnp.zeros_like(cum0)
    zeros5 = jnp.zeros((5, cum0.shape[1]), F32)

    def rows(a, b, d):
        return jnp.concatenate([a, b, d, zeros5], axis=0)

    per_head = jnp.concatenate(
        [
            rows(jnp.exp(cum0), jnp.exp(cum1), jnp.exp(cum2)),
            rows(step[0:1], step[1:2], step[2:3]),
            rows(none, jnp.exp(cum1 - cum0) * step[0:1], jnp.exp(cum2 - cum1) * step[1:2]),
            rows(none, none, jnp.exp(cum2 - cum0) * step[0:1]),
            rows(dpw[...], dpw[...], dpw[...]),
        ],
        axis=0,
    )
    heads = per_head.shape[1]
    lanes = heads * 64
    to_head = iota((heads, lanes), 1) - iota((heads, lanes), 0) * 64
    expand = one_hot((to_head >= 0) & (to_head < 64))
    hi, mid, lo = split3(per_head)
    wide_heads = dot(hi, expand) + dot(mid, expand) + dot(lo, expand)
    carry_w, mix0, mix1, mix2, direct = (wide_heads[i * 8 : (i + 1) * 8] for i in range(5))

    start = jnp.clip(acc_s[0] - 1, 0, 2)
    ones3 = jnp.ones((3, 64), BF16)
    for g in range(2):
        at_g = slice(g * 1024, (g + 1) * 1024)
        s0 = st[start, at_g, :]
        s_hi = s0.astype(BF16)
        s_lo = (s0 - s_hi.astype(F32)).astype(BF16)
        s0cat[at_g, :] = jnp.concatenate([s_hi, s_lo], axis=1)
        for j in range(3):
            line = carry_w[j : j + 1, at_g]
            l_hi, l_mid, l_lo = split3(line)
            stack = jnp.concatenate([l_hi.astype(F32), l_mid.astype(F32), l_lo.astype(F32)], axis=0).astype(BF16)
            snew[j, at_g, :] = dot_tn(stack, ones3) * s0

    def in_order(v):
        a, b = v[:, 0, :], v[:, 1, :]
        return jnp.concatenate(
            [a[:, :1024], b[:, :1024], a[:, 1024:1088], b[:, 1024:1088], a[:, 1088:], b[:, 1088:]], axis=1
        )

    kept = in_order(hist[...].astype(F32))
    taps = in_order(tap[...].astype(F32))
    accepted = acc_s[0]
    context = jnp.where(accepted == 1, kept[1:4], jnp.where(accepted == 2, kept[2:5], kept[3:6]))
    context = jnp.concatenate([context, jnp.zeros((5, context.shape[1]), F32)], axis=0)

    def send_near(to, _):
        pl.semaphore_wait(may.at[to], 1)
        direct_slice(to)

        @pl.when(to + 8 < NZ)
        def _():
            slot = o - to + 8
            copy_slice(nst.at[chip(to + 8)], rel0.at[slot], asend, r0recv.at[slot], to).start()

        return 0

    lax.fori_loop(o + 1, jnp.minimum(o + 9, NZ), send_near, 0)

    def pass_on(rel, slot, source, sems, recv, to):
        copy_slice(rel.at[slot], rel.at[slot], asend, recv.at[slot], to).wait_recv()
        copy_slice(rel.at[slot], xs.at[chip(source)], sems.at[slot], arecv, to).start()

    @pl.when(o + 8 < NZ)
    def _():
        def pass_right(slot, _):
            pass_on(rel0, slot, o - 8 + slot, r0send, r0recv, o + 8)
            return 0

        lax.fori_loop(jnp.maximum(8 - o, 0), 8, pass_right, 0)

    def send_far(to, _):
        pl.semaphore_wait(may.at[to], 1)
        direct_slice(to)
        return 0

    lax.fori_loop(o + 17, 24, send_far, 0)

    @pl.when(o + 24 < NZ)
    def _():
        send_far(o + 24, 0)

        def pass_left(slot, _):
            pass_on(rel1, slot, o + 1 + slot, r1send, r1recv, o + 24)
            return 0

        lax.fori_loop(0, 7, pass_left, 0)

    lax.fori_loop(o + 25, NZ, send_far, 0)

    for cp in shares:
        cp.wait_recv()
    pltpu.make_async_remote_copy(
        src_ref=nst.at[0 : NZ - 1], dst_ref=xs.at[0 : NZ - 1], send_sem=asend, recv_sem=arecv, device_id=partner,
        device_id_type=MESH,
    ).wait_recv()
    x_rows = jnp.concatenate([xs[k].astype(F32) for k in range(NZ)], axis=0).astype(BF16)
    to_row = iota((128, 32), 0)
    from_row = iota((128, 32), 1)
    packed_row = lax.rem(to_row, 16)
    spread = one_hot((to_row // 16 == from_row // 4) & (packed_row // CB == lax.rem(from_row, 4)) & (packed_row < 3 * CB))
    x_all = jnp.concatenate([dot(spread, x_rows[i * 32 : (i + 1) * 32]) for i in range(4)], axis=0).astype(BF16)
    block_of = lax.rem(lax.rem(iota((NZ * 16, 128), 0), 16), CB)
    zero = jnp.zeros_like(x_all)
    stacked = jnp.concatenate([jnp.where(block_of == cb, x_all, zero) for cb in range(CB)], axis=1)
    for n0, n1 in ((0, 256), (256, 512), (512, 768), (768, 896)):
        part[:, :, n0:n1] = dot(stacked, w2[:, n0:n1]).astype(BF16).reshape(NZ, 16, n1 - n0)

    def member(delta, hop, head, slot):
        pltpu.make_async_remote_copy(
            src_ref=part.at[at(delta)], dst_ref=mem.at[head // 4, slot], send_sem=msend, recv_sem=mrecv.at[head // 4],
            device_id={"z": at(hop)}, device_id_type=MESH,
        ).start()

    def members(head):
        member((head + 1) % NZ, 1, head, 0)
        member((head - 1) % NZ, -1, head, 1)
        if head < 16:
            member(head + 2, 2, head, 2)
        if head > 16:
            member(head - 2, -2, head, 2)
        if head == 0:
            member(NZ - 2, -2, head, 3)

    def quad(head):
        count = {0: 4, 16: 2}.get(head, 3)
        pltpu.make_async_remote_copy(
            src_ref=mem.at[head // 4, 0:count], dst_ref=mem.at[head // 4, 0:count], send_sem=msend,
            recv_sem=mrecv.at[head // 4], device_id=partner, device_id_type=MESH,
        ).wait_recv()
        total = part[at(head)].astype(F32)
        for slot in range(count):
            total += mem[head // 4, slot].astype(F32)
        return total

    def chain(step_at, hop):
        return pltpu.make_async_remote_copy(
            src_ref=cout.at[step_at], dst_ref=cin.at[step_at], send_sem=csend.at[step_at], recv_sem=crecv.at[step_at],
            device_id={"z": at(hop)}, device_id_type=MESH,
        )

    right = [chain(i, 4) for i in range(4)]
    left = [chain(4 + i, -4) for i in range(3)]
    for head in (16, 12, 20):
        members(head)
    cout[0] = quad(16).astype(BF16)
    right[0].start()
    cout[4] = quad(20).astype(BF16)
    left[0].start()
    for head in (8, 24):
        members(head)
    total = quad(12)
    right[0].wait_recv()
    cout[1] = (total + cin[0].astype(F32)).astype(BF16)
    right[1].start()
    total = quad(24)
    left[0].wait_recv()
    cout[5] = (total + cin[4].astype(F32)).astype(BF16)
    left[1].start()
    for head in (4, 28):
        members(head)
    total = quad(8)
    right[1].wait_recv()
    cout[2] = (total + cin[1].astype(F32)).astype(BF16)
    right[2].start()
    total = quad(28)
    left[1].wait_recv()
    cout[6] = (total + cin[5].astype(F32)).astype(BF16)
    left[2].start()
    members(0)
    total = quad(4)
    right[2].wait_recv()
    cout[3] = (total + cin[2].astype(F32)).astype(BF16)
    right[3].start()
    total = quad(0)
    left[2].wait_recv()
    total += cin[6].astype(F32)
    right[3].wait_recv()
    total += cin[3].astype(F32)
    owned = total.astype(BF16)

    urow = iota((8 * CB, 16), 0)
    ucol = iota((8 * CB, 16), 1)
    ublk, uj = urow // 8, lax.rem(urow, 8) - 3
    unpack = one_hot((ucol == uj * CB + ublk) & (uj >= 0) & (uj < 3))
    wide_rows = dot(unpack, owned)
    fresh = jnp.concatenate([wide_rows[cb * 8 : (cb + 1) * 8] for cb in range(CB)], axis=1)
    span = fresh[:, :2304] + context
    gate = pltpu.roll(fresh[:, 2304:4352], 5, 0)

    conv = span * taps[0:1]
    for k in range(1, 4):
        conv += pltpu.roll(span, 8 - k, 0) * taps[k : k + 1]
    live = iota(conv.shape, 0) < 3
    act = jnp.where(live, silu(conv), 0.0)
    x = act[:, :2048]
    inject = act[:, 2048:2176]
    readout = act[:, 2176:2304]
    x1 = pltpu.roll(x, 1, 0)
    x2 = pltpu.roll(x, 2, 0)
    i1 = pltpu.roll(inject, 1, 0)
    i2 = pltpu.roll(inject, 2, 0)

    outs = []
    for g in range(2):
        at_g = slice(g * 1024, (g + 1) * 1024)
        half = slice(g * 64, (g + 1) * 64)
        rd = readout[:, half]
        r_hi = rd.astype(BF16)
        r_lo = (rd - r_hi.astype(F32)).astype(BF16)
        both = jnp.concatenate([r_hi, r_hi], axis=1)
        low = jnp.concatenate([r_lo, jnp.zeros_like(r_lo)], axis=1)
        s_part = s0cat[at_g, :]
        first = dot_nt(both, s_part) + dot_nt(low, s_part)
        d0 = jnp.sum(rd * inject[:, half], axis=1, keepdims=True)
        d1 = jnp.sum(rd * i1[:, half], axis=1, keepdims=True)
        d2 = jnp.sum(rd * i2[:, half], axis=1, keepdims=True)
        response = (
            carry_w[:, at_g] * first
            + mix0[:, at_g] * x[:, at_g] * d0
            + mix1[:, at_g] * x1[:, at_g] * d1
            + mix2[:, at_g] * x2[:, at_g] * d2
            + direct[:, at_g] * x[:, at_g]
        )
        gated = jnp.where(live[:, :1024], response * silu(gate[:, at_g]), 0.0)
        norm = lax.rsqrt(jnp.sum(gated * gated, axis=1, keepdims=True) * (1.0 / 1024) + EPS)
        outs.append(gated * norm * gns[:, at_g])
    gated = jnp.concatenate(outs, axis=1)

    stack = jnp.concatenate([gated[:, cb * GBLK : (cb + 1) * GBLK] for cb in range(CB)], axis=0).astype(BF16)
    prow = iota((16, 8 * CB), 0)
    pcol = iota((16, 8 * CB), 1)
    packed = dot(one_hot(prow == lax.rem(pcol, 8) * CB + pcol // 8), stack)
    rest = gated[:, CB * GBLK :]
    last = jnp.concatenate([rest[j : j + 1] for j in range(3)], axis=1)
    packed = jnp.where(iota((16, GBLK), 0) == 15, jnp.broadcast_to(last, (16, GBLK)), packed)
    gown[...] = packed.astype(BF16)
    gath[z] = packed.astype(BF16)

    def share(src_ref, slot, hop, recv):
        pltpu.make_async_remote_copy(
            src_ref=src_ref, dst_ref=gath.at[slot], send_sem=gsend, recv_sem=recv, device_id={"z": at(hop)},
            device_id_type=MESH,
        ).start()

    for k in (4, 3, 5, 2, 6, 1, 7):
        share(gown, z, 4 * k, grecv.at[k])
    for hop in (-2, -1, 1, 2):
        share(gown, z, hop, nrecv)

    for g in range(2):
        at_g = slice(g * 1024, (g + 1) * 1024)
        half = slice(g * 64, (g + 1) * 64)
        b8 = inject[:, half]
        b_hi = b8.astype(BF16).astype(F32)
        b_lo = b8 - b_hi
        rhs = jnp.concatenate([b_hi, b_lo, b_hi], axis=0).astype(BF16)
        live0 = iota((8, 1024), 0)
        for j in range(3):
            coef = jnp.zeros((8, 1024), F32)
            for i in range(j + 1):
                mix = (mix0, mix1, mix2)[j - i]
                coef = jnp.where(live0 == i, mix[j : j + 1, at_g], coef)
            a8 = coef * x[:, at_g]
            a_hi = a8.astype(BF16).astype(F32)
            a_lo = a8 - a_hi
            lhs = jnp.concatenate([a_hi, a_hi, a_lo], axis=0).astype(BF16)
            snew[j, at_g, :] += dot_tn(lhs, rhs)
    groups = [
        jnp.concatenate(
            [
                span[:, g * 1024 : (g + 1) * 1024],
                span[:, 2048 + g * 64 : 2048 + (g + 1) * 64],
                span[:, 2176 + g * 64 : 2176 + (g + 1) * 64],
            ],
            axis=1,
        )
        for g in range(2)
    ]
    for i in range(6):
        tail_o[i] = jnp.concatenate([groups[0][i : i + 1], groups[1][i : i + 1]], axis=0).astype(BF16)

    for k in (1, 7, 2, 6, 3, 5, 4):
        slot = at(-4 * k)
        pltpu.make_async_remote_copy(
            src_ref=gown, dst_ref=gath.at[slot], send_sem=gsend, recv_sem=grecv.at[k], device_id=partner, device_id_type=MESH
        ).wait_recv()
        for hop in (-1, 1) + ((2,) if k < 4 else (-2,) if k > 4 else ()):
            share(gath.at[slot], slot, hop, nrecv)
    pltpu.make_async_remote_copy(
        src_ref=gath.at[0:24], dst_ref=gath.at[0:24], send_sem=gsend, recv_sem=nrecv, device_id=partner, device_id_type=MESH
    ).wait_recv()

    srow = iota((32 * CB, 128), 0)
    scol = iota((32 * CB, 128), 1)
    m, scb = lax.rem(srow, 32), srow // 32
    select = one_hot((m // 4 == scol // 16) & (lax.rem(scol, 16) == lax.rem(m, 4) * CB + scb) & (lax.rem(m, 4) < 3))
    m2 = iota((32, 128), 0)
    c2 = iota((32, 128), 1)
    pick = [one_hot((m2 // 4 == c2 // 16) & (lax.rem(c2, 16) == 15) & (lax.rem(m2, 4) == j)) for j in range(3)]
    inputs = []
    for tb in range(4):
        block = gath[tb * 8 : (tb + 1) * 8].reshape(128, GBLK)
        y = dot(select, block)
        tail = sum(dot(pick[j], block[:, j * 128 : (j + 1) * 128]) for j in range(3))
        inputs.append(jnp.concatenate([y[cb * 32 : (cb + 1) * 32] for cb in range(CB)] + [tail], axis=1).astype(BF16))
    full = jnp.concatenate(inputs, axis=0)
    own_cols = dot_nt(full, wo[...]).astype(BF16)
    partner_cols = dot_nt(full, wop[...]).astype(BF16)
    for tb in range(4):
        fst[0, tb] = own_cols[tb * 32 : (tb + 1) * 32]
        fst[1, tb] = partner_cols[tb * 32 : (tb + 1) * 32]

    finals = []
    for i, (dc, dt) in enumerate(others):
        to = lax.rem(t + dt, n_tp)
        finals.append(
            pltpu.make_async_remote_copy(
                src_ref=fst.at[dc, to], dst_ref=fin.at[c, t], send_sem=fsend.at[i], recv_sem=frecv.at[i],
                device_id={"c": lax.rem(c + dc, 2), "tp": to}, device_id_type=MESH,
            )
        )
    for cp in finals:
        cp.start()
    fin[c, t] = fst[0, t]
    for cp in finals:
        cp.wait_recv()
    totals = []
    for k in range(2):
        total = fin[k, 0].astype(F32)
        for i in range(1, 4):
            total += fin[k, i].astype(F32)
        totals.append(total.astype(BF16))
    trow = iota((48, 32), 0)
    tcol = iota((48, 32), 1)
    want = 4 * (lax.rem(trow, 16) // 2) + trow // 16
    arranged = sum(dot(one_hot((lax.rem(trow, 2) == k) & (tcol == want)), totals[k]) for k in range(2))
    for j in range(3):
        mixed_o[j] = arranged[j * 16 : (j + 1) * 16].astype(BF16)

    @pl.when(o + 8 < NZ)
    def _():
        def left_right(slot, _):
            copy_slice(rel0.at[slot], rel0.at[slot], r0send.at[slot], arecv, o + 8).wait_send()
            return 0

        lax.fori_loop(jnp.maximum(8 - o, 0), 8, left_right, 0)

    @pl.when(o + 24 < NZ)
    def _():
        def left_left(slot, _):
            copy_slice(rel1.at[slot], rel1.at[slot], r1send.at[slot], arecv, o + 24).wait_send()
            return 0

        lax.fori_loop(0, 7, left_left, 0)

    for cp in shares:
        cp.wait_send()
    for cp in right + left:
        cp.wait_send()
    for cp in finals:
        cp.wait_send()
    for ref, count, sem in ((xs, NZ - 1, asend), (part, 24, msend), (gath, NZ - 1, gsend)):
        pltpu.make_async_remote_copy(
            src_ref=ref.at[0:count], dst_ref=ref.at[0:count], send_sem=sem, recv_sem=arecv, device_id=partner,
            device_id_type=MESH,
        ).wait_send()


def store(mixed, states, tail, mixed_o, states_o, tail_o, sem):
    copies = [
        pltpu.make_async_copy(src, dst, sem.at[i])
        for i, (src, dst) in enumerate(((states, states_o), (tail, tail_o), (mixed, mixed_o)))
    ]
    for cp in copies:
        cp.start()
    for cp in copies:
        cp.wait()


def local(
    tokens,
    input_norm_scale,
    head_input_matrix,
    output_gate_matrix,
    group_input_matrix,
    group_readout_matrix,
    step_size_matrix,
    step_size_bias,
    log_decay_rate,
    direct_path_weight,
    convolution_tap_weight,
    convolution_history_rows,
    per_proposal_states,
    accepted,
    proposal_extra_decay,
    group_norm_scale,
    output_projection_matrix,
):
    width = tokens.shape[2]
    heads = step_size_bias.shape[0]
    channels = heads * 64
    dma = pltpu.SemaphoreType.DMA
    any_space = pl.BlockSpec(memory_space=pl.ANY)
    smem = pl.BlockSpec(memory_space=pltpu.SMEM)
    vmem = pl.BlockSpec(memory_space=pltpu.VMEM)
    mixed, states, tail = pl.pallas_call(
        kernel,
        name="mixer",
        out_shape=(
            pltpu.VMEM((3, 16, 64), BF16),
            pltpu.VMEM((3, channels, 64), F32),
            pltpu.VMEM((6, 2, 1152), BF16),
        ),
        in_specs=[any_space] * 13 + [smem] + [any_space] * 3,
        out_specs=(vmem, vmem, vmem),
        scratch_shapes=[
            pltpu.VMEM((3, width), BF16),
            pltpu.VMEM((1, width), F32),
            pltpu.VMEM((heads, width), BF16),
            pltpu.VMEM((1, heads), F32),
            pltpu.VMEM((1, heads), F32),
            pltpu.VMEM((1, heads), F32),
            pltpu.VMEM((4, 2, 1152), BF16),
            pltpu.VMEM((6, 2, 1152), BF16),
            pltpu.VMEM((3, channels, 64), F32),
            pltpu.VMEM((3, 1, heads), F32),
            pltpu.VMEM((1, channels), F32),
            pltpu.VMEM((64, channels), BF16),
            pltpu.VMEM((64, channels), BF16),
            pltpu.VMEM((CB * 128, BLK), BF16),
            pltpu.VMEM((NZ, 4, 128), BF16),
            pltpu.VMEM((NZ, 4, 128), BF16),
            pltpu.VMEM((NZ, 16, BLK), BF16),
            pltpu.VMEM((8, 4, 16, BLK), BF16),
            pltpu.VMEM((7, 16, BLK), BF16),
            pltpu.VMEM((7, 16, BLK), BF16),
            pltpu.VMEM((NZ, 16, GBLK), BF16),
            pltpu.VMEM((16, GBLK), BF16),
            pltpu.VMEM((2, 4, 32, 64), BF16),
            pltpu.VMEM((2, 4, 32, 64), BF16),
            pltpu.VMEM((channels, 128), BF16),
            dma((12 + len(PIECES),)),
            dma((len(PIECES) + 1,)),
            dma((len(PIECES) + 1,)),
            dma,
            dma,
            dma,
            dma((8,)),
            dma((7,)),
            dma((7,)),
            dma,
            dma((8,)),
            dma,
            dma((7,)),
            dma((7,)),
            pltpu.VMEM((8, 4, 128), BF16),
            pltpu.VMEM((7, 4, 128), BF16),
            dma((8,)),
            dma((8,)),
            dma((7,)),
            dma((7,)),
            pltpu.SemaphoreType.REGULAR((NZ,)),
        ],
        compiler_params=pltpu.CompilerParams(
            collective_id=0, has_side_effects=True, vmem_limit_bytes=56 * 1024 * 1024
        ),
    )(
        tokens,
        input_norm_scale.reshape(1, width),
        head_input_matrix,
        output_gate_matrix,
        group_input_matrix,
        group_readout_matrix,
        step_size_matrix.T,
        step_size_bias.reshape(1, heads),
        log_decay_rate.reshape(1, heads),
        direct_path_weight.reshape(1, heads),
        convolution_tap_weight,
        convolution_history_rows,
        per_proposal_states.reshape(3, channels, 64),
        accepted,
        proposal_extra_decay.transpose(1, 0, 2),
        group_norm_scale.reshape(1, channels),
        output_projection_matrix.T,
    )
    mixed, states, tail = pl.pallas_call(
        store,
        name="store",
        out_shape=(
            jax.ShapeDtypeStruct((3, 16, 64), BF16),
            jax.ShapeDtypeStruct((3, channels, 64), F32),
            jax.ShapeDtypeStruct((6, 2, 1152), BF16),
        ),
        in_specs=[pl.BlockSpec(memory_space=pltpu.VMEM)] * 3,
        out_specs=(any_space,) * 3,
        scratch_shapes=[dma((3,))],
    )(*(pltpu.with_memory_space_constraint(v, pltpu.VMEM) for v in (mixed, states, tail)))
    mixed = mixed.transpose(1, 0, 2)
    states = states.reshape(1, 3, heads, 64, 64)
    tail = tail[None]
    return mixed, states, tail


def solution(mesh):
    ring = mesh.shape["kv"] // 2
    assert ring == NZ and mesh.shape["tp"] == 4
    finer = Mesh(
        mesh.devices.reshape(mesh.shape["grp"], ring, 2, mesh.shape["tp"]),
        ("grp", "z", "c", "tp"),
    )
    return jax.shard_map(
        local,
        mesh=finer,
        in_specs=(
            P(GRP_KV, None, None),
            P(),
            P(KV, "tp"),
            P(KV, "tp"),
            P(KV, "tp"),
            P(KV, "tp"),
            P(None, "tp"),
            P("tp"),
            P("tp"),
            P("tp"),
            P(None, "tp", None),
            P(GRP_KV, None, "tp", None),
            P(GRP_KV, None, "tp", None, None),
            P(GRP_KV),
            P(GRP_KV, None, "tp"),
            P("tp"),
            P("tp", KV),
        ),
        out_specs=(
            P(("grp", "tp"), None, KV),
            P(GRP_KV, None, "tp", None, None),
            P(GRP_KV, None, "tp", None),
        ),
        check_vma=False,
    )
```

```python
import functools

import jax
import jax.numpy as jnp
from jax import lax
from jax.experimental import pallas as pl
from jax.experimental.pallas import tpu as pltpu
from jax.sharding import Mesh
from jax.sharding import PartitionSpec as P

MESH = pl.DeviceIdType.MESH
EPS = 1e-06
F32 = jnp.float32
BF16 = jnp.bfloat16

KV = ("z", "c")
GRP_KV = ("grp", "z", "c")

STAGES = (0, 16, 24, 32)
LAST = 28
CLOSE = 26
NZ = 32
BLK = 896
CB = 5
GBLK = 384


def iota(shape, dim):
    return lax.broadcasted_iota(jnp.int32, shape, dim)


def split3(v):
    hi = v.astype(BF16)
    rest = v - hi.astype(F32)
    mid = rest.astype(BF16)
    lo = (rest - mid.astype(F32)).astype(BF16)
    return hi, mid, lo


def dot(a, b):
    return jnp.dot(a, b, preferred_element_type=F32)


def dot_nt(a, b):
    return lax.dot_general(a, b, (((1,), (1,)), ((), ())), preferred_element_type=F32)


def dot_tn(a, b):
    return lax.dot_general(a, b, (((0,), (0,)), ((), ())), preferred_element_type=F32)


def silu(v):
    return v / (1.0 + jnp.exp(-v))


def one_hot(cond):
    return jnp.where(cond, 1.0, 0.0).astype(BF16)


PIECES = (
    (0, 0, 896, 0, 0),
    (0, 896, 896, 1, 0),
    (0, 1792, 256, 2, 0),
    (2, 0, 128, 2, 256),
    (3, 0, 128, 2, 384),
    (1, 0, 384, 2, 512),
    (1, 384, 896, 3, 0),
    (1, 1280, 768, 4, 0),
)


def kernel(
    tok_h, ins_h, wh_h, wg_h, wi_h, wr_h, ws_h, bias_h, ldr_h, dpw_h, tap_h, hist_h, st_h, acc_h, ped_h, gns_h, wo_h,
    mixed_o, snew, tail_o,
    tok, ins, ws, bias, ldr, dpw, tap, hist, st, ped, gns, wo, wop,
    w2, nst, xs, part, mem, cout, cin, gath, gown, fin, fst, s0cat,
    lsem, wsend, wrecv, asend, arecv, msend, mrecv, csend, crecv, gsend, grecv, nrecv, fsend, frecv, rel0, rel1, r0send, r0recv, r1send, r1recv, may, acc_s, rel2, r2send, r2recv,
):
    z = lax.axis_index("z")
    c = lax.axis_index("c")
    t = lax.axis_index("tp")
    n_tp = lax.axis_size("tp")

    o = lax.rem(z + NZ - 1, NZ)

    def at(offset):
        return lax.rem(z + (offset + NZ) % NZ, NZ)

    def place_of(offset):
        return lax.rem(o + (offset + NZ) % NZ, NZ)

    def chip(place):
        return lax.rem(place + 1, NZ)

    def stage_of(place):
        return jnp.where(place < STAGES[1], 0, jnp.where(place < STAGES[2], 1, 2))

    pairs = [
        (tok_h.at[0], tok), (ins_h, ins), (ws_h, ws), (bias_h, bias), (ldr_h, ldr), (dpw_h, dpw), (tap_h, tap),
        (hist_h.at[0], hist), (ped_h, ped), (gns_h, gns), (st_h, st), (wo_h, wo), (acc_h, acc_s),
    ]
    loads = [pltpu.make_async_copy(src, dst, lsem.at[i]) for i, (src, dst) in enumerate(pairs)]
    sources = (wh_h, wg_h, wi_h, wr_h)
    mine = pl.multiple_of(c * 64, 64)
    for i, (source, first, count, row, lane) in enumerate(PIECES):
        loads.append(
            pltpu.make_async_copy(
                sources[source].at[:, first : first + count],
                w2.at[pl.ds(pl.multiple_of(row * 128 + mine, 64), 64), lane : lane + count],
                lsem.at[len(pairs) + i],
            )
        )
    for cp in loads:
        cp.start()

    barrier = pltpu.get_barrier_semaphore()

    def greet(to, _):
        pl.semaphore_signal(barrier, inc=1, device_id={"z": chip(to)}, device_id_type=MESH)
        return 0

    lax.fori_loop(o + 1, NZ, greet, 0)
    others = [(dc, dt) for dc in range(2) for dt in range(n_tp) if (dc, dt) != (0, 0)]
    for dc, dt in others:
        pl.semaphore_signal(
            barrier, inc=1, device_id={"c": lax.rem(c + dc, 2), "tp": lax.rem(t + dt, n_tp)}, device_id_type=MESH
        )

    pl.semaphore_wait(barrier, o + len(others))

    def tell(k, _):
        to = chip(o - k)

        usual = (k <= 8) | (k >= 24) | ((k >= 17) & (o < 24))
        last = (k == LAST) | (k <= o - CLOSE)

        @pl.when(((o < LAST) & usual) | ((o >= LAST) & last))
        def _():
            pl.semaphore_signal(may.at[o], inc=1, device_id={"z": to}, device_id_type=MESH)

        return 0

    lax.fori_loop(1, o + 1, tell, 0)

    loads[0].wait()
    loads[1].wait()
    wide = tok[...].astype(F32)
    scale = lax.rsqrt(jnp.sum(wide * wide, axis=-1, keepdims=True) * (1.0 / wide.shape[1]) + EPS)
    normed = (wide * scale * ins[...]).astype(BF16)
    padded = jnp.concatenate([normed.astype(F32), jnp.zeros((1, normed.shape[1]), F32)], axis=0).astype(BF16)
    for k in range(NZ):
        nst[k] = padded[:, k * 128 : (k + 1) * 128]

    def copy_slice(src_ref, dst_ref, send_sem, recv_sem, to):
        return pltpu.make_async_remote_copy(
            src_ref=src_ref, dst_ref=dst_ref, send_sem=send_sem, recv_sem=recv_sem, device_id={"z": chip(to)},
            device_id_type=MESH,
        )

    def direct_slice(to):
        copy_slice(nst.at[chip(to)], xs.at[o], asend, arecv.at[stage_of(o)], to).start()

    def send_back(to, _):
        direct_slice(to)
        return 0

    lax.fori_loop(0, o, send_back, 0)

    def send_by_first(to, _):
        relay = to - 24
        copy_slice(nst.at[chip(to)], rel1.at[o - relay - 1], asend, r1recv.at[o - relay - 1], relay).start()
        return 0

    lax.fori_loop(jnp.maximum(o + 17, 24), jnp.minimum(o + 24, LAST), send_by_first, 0)

    def send_by_wrap(relay, _):
        copy_slice(nst.at[chip(relay + LAST)], rel2.at[o], asend, r2recv.at[o], relay).start()
        return 0

    @pl.when(o < CLOSE)
    def _():
        lax.fori_loop(0, jnp.minimum(o, NZ - LAST), send_by_wrap, 0)

    xs[o] = nst[z]

    partner = {"c": 1 - c}
    shares = []
    for i, (source, first, count, row, lane) in enumerate(PIECES):
        shares.append(
            pltpu.make_async_remote_copy(
                src_ref=sources[source].at[:, first : first + count],
                dst_ref=w2.at[pl.ds(pl.multiple_of(row * 128 + mine, 64), 64), lane : lane + count],
                send_sem=wsend.at[i], recv_sem=wrecv.at[i], device_id=partner, device_id_type=MESH,
            )
        )
    shares.append(
        pltpu.make_async_remote_copy(
            src_ref=wo_h, dst_ref=wop, send_sem=wsend.at[len(PIECES)], recv_sem=wrecv.at[len(PIECES)],
            device_id=partner, device_id_type=MESH,
        )
    )
    for cp in shares:
        cp.start()

    for cp in loads[2:]:
        cp.wait()
    w2[4 * 128 :, 768:] = jnp.zeros((128, 128), BF16)
    step_raw = dot_nt(normed, ws[...])
    raw = step_raw + bias[...]
    step = jnp.maximum(raw, 0.0) + jnp.log1p(jnp.exp(-jnp.abs(raw)))
    decay = jnp.exp(ldr[...]) * step
    cum0 = ped[0] - decay[0:1]
    cum1 = cum0 + (ped[1] - decay[1:2])
    cum2 = cum1 + (ped[2] - decay[2:3])
    none = jnp.zeros_like(cum0)
    zeros5 = jnp.zeros((5, cum0.shape[1]), F32)

    def rows(a, b, d):
        return jnp.concatenate([a, b, d, zeros5], axis=0)

    per_head = jnp.concatenate(
        [
            rows(jnp.exp(cum0), jnp.exp(cum1), jnp.exp(cum2)),
            rows(step[0:1], step[1:2], step[2:3]),
            rows(none, jnp.exp(cum1 - cum0) * step[0:1], jnp.exp(cum2 - cum1) * step[1:2]),
            rows(none, none, jnp.exp(cum2 - cum0) * step[0:1]),
            rows(dpw[...], dpw[...], dpw[...]),
        ],
        axis=0,
    )
    heads = per_head.shape[1]
    lanes = heads * 64
    to_head = iota((heads, lanes), 1) - iota((heads, lanes), 0) * 64
    expand = one_hot((to_head >= 0) & (to_head < 64))
    hi, mid, lo = split3(per_head)
    wide_heads = dot(hi, expand) + dot(mid, expand) + dot(lo, expand)
    carry_w, mix0, mix1, mix2, direct = (wide_heads[i * 8 : (i + 1) * 8] for i in range(5))

    start = jnp.clip(acc_s[0] - 1, 0, 2)
    ones3 = jnp.ones((3, 64), BF16)
    for g in range(2):
        at_g = slice(g * 1024, (g + 1) * 1024)
        s0 = st[start, at_g, :]
        s_hi = s0.astype(BF16)
        s_lo = (s0 - s_hi.astype(F32)).astype(BF16)
        s0cat[at_g, :] = jnp.concatenate([s_hi, s_lo], axis=1)
        for j in range(3):
            line = carry_w[j : j + 1, at_g]
            l_hi, l_mid, l_lo = split3(line)
            stack = jnp.concatenate([l_hi.astype(F32), l_mid.astype(F32), l_lo.astype(F32)], axis=0).astype(BF16)
            snew[j, at_g, :] = dot_tn(stack, ones3) * s0

    def in_order(v):
        a, b = v[:, 0, :], v[:, 1, :]
        return jnp.concatenate(
            [a[:, :1024], b[:, :1024], a[:, 1024:1088], b[:, 1024:1088], a[:, 1088:], b[:, 1088:]], axis=1
        )

    kept = in_order(hist[...].astype(F32))
    taps = in_order(tap[...].astype(F32))
    accepted = acc_s[0]
    context = jnp.where(accepted == 1, kept[1:4], jnp.where(accepted == 2, kept[2:5], kept[3:6]))
    context = jnp.concatenate([context, jnp.zeros((5, context.shape[1]), F32)], axis=0)

    to_row = iota((128, 32), 0)
    from_row = iota((128, 32), 1)
    packed_row = lax.rem(to_row, 16)
    spread = one_hot((to_row // 16 == from_row // 4) & (packed_row // CB == lax.rem(from_row, 4)) & (packed_row < 3 * CB))

    def member(delta, hop, head, slot, when):
        dest = place_of(delta)

        @pl.when(when(stage_of(dest), o + hop < 0))
        def _():
            pltpu.make_async_remote_copy(
                src_ref=part.at[dest], dst_ref=mem.at[head // 4, slot], send_sem=msend, recv_sem=mrecv.at[head // 4],
                device_id={"z": at(hop)}, device_id_type=MESH,
            ).start()

    def members(head, when):
        member((head + 1) % NZ, 1, head, 0, when)
        member((head - 1) % NZ, -1, head, 1, when)
        if head < 16:
            member(head + 2, 2, head, 2, when)
        if head > 16:
            member(head - 2, -2, head, 2, when)
        if head == 0:
            member(NZ - 2, -2, head, 3, when)

    def arrived(stage):
        first, last = STAGES[stage], STAGES[stage + 1]

        def wait(count):
            pltpu.make_async_remote_copy(
                src_ref=xs.at[0:count], dst_ref=xs.at[0:count], send_sem=asend, recv_sem=arecv.at[stage],
                device_id=partner, device_id_type=MESH,
            ).wait_recv()

        @pl.when(stage_of(o) == stage)
        def _():
            wait(last - first - 1)

        @pl.when(stage_of(o) != stage)
        def _():
            wait(last - first)

    def multiply(stage):
        first, last = STAGES[stage], STAGES[stage + 1]
        rows = (last - first) * 16
        x_rows = jnp.concatenate([xs[k].astype(F32) for k in range(first, last)], axis=0).astype(BF16)
        x_all = jnp.concatenate([dot(spread, x_rows[i : i + 32]) for i in range(0, x_rows.shape[0], 32)], axis=0)
        x_all = x_all.astype(BF16)
        block_of = lax.rem(lax.rem(iota((rows, 128), 0), 16), CB)
        zero = jnp.zeros_like(x_all)
        stacked = jnp.concatenate([jnp.where(block_of == cb, x_all, zero) for cb in range(CB)], axis=1)
        for n0, n1 in ((0, 256), (256, 512), (512, 768), (768, 896)):
            part[first:last, :, n0:n1] = dot(stacked, w2[:, n0:n1]).astype(BF16).reshape(last - first, 16, n1 - n0)

    def send_near(to, _):
        pl.semaphore_wait(may.at[to], 1)
        direct_slice(to)

        @pl.when(to + 8 < LAST)
        def _():
            slot = o - to + 8
            copy_slice(nst.at[chip(to + 8)], rel0.at[slot], asend, r0recv.at[slot], to).start()

        return 0

    lax.fori_loop(o + 1, jnp.minimum(o + 9, jnp.where(o < CLOSE, LAST, NZ)), send_near, 0)
    lax.fori_loop(o + 1, NZ - LAST, send_by_wrap, 0)

    def pass_on(rel, slot, source, sems, recv, to):
        copy_slice(rel.at[slot], rel.at[slot], asend, recv.at[slot], to).wait_recv()
        copy_slice(rel.at[slot], xs.at[source], sems.at[slot], arecv.at[stage_of(source)], to).start()

    @pl.when(o + 8 < LAST)
    def _():
        def pass_right(slot, _):
            pass_on(rel0, slot, o - 8 + slot, r0send, r0recv, o + 8)
            return 0

        lax.fori_loop(jnp.maximum(8 - o, 0), 8, pass_right, 0)

    def send_far(to, _):
        pl.semaphore_wait(may.at[to], 1)
        direct_slice(to)
        return 0

    lax.fori_loop(o + 17, STAGES[2], send_far, 0)

    for cp in shares:
        cp.wait_recv()
    arrived(0)
    multiply(0)
    for head in (16, 12, 20, 8, 24, 4, 28, 0):
        members(head, lambda stage, edge: (o < STAGES[2]) & (stage == 0) & ~edge)

    @pl.when(o + 24 < LAST)
    def _():
        send_far(o + 24, 0)

        def pass_left(slot, _):
            pass_on(rel1, slot, o + 1 + slot, r1send, r1recv, o + 24)
            return 0

        lax.fori_loop(0, 7, pass_left, 0)

    lax.fori_loop(o + 25, LAST, send_far, 0)

    @pl.when(o + LAST < NZ)
    def _():
        send_far(o + LAST, 0)

        def pass_wrap(slot, _):
            @pl.when(slot != o)
            def _():
                pass_on(rel2, slot, slot, r2send, r2recv, o + LAST)

            return 0

        lax.fori_loop(0, CLOSE, pass_wrap, 0)


    arrived(1)
    multiply(1)
    for head in (16, 12, 20, 8, 24, 4, 28, 0):
        members(head, lambda stage, edge: (o < STAGES[2]) & (stage == 1) & ~edge)

    arrived(2)
    multiply(2)

    def late(stage, edge):
        return (o >= STAGES[2]) | (stage == 2) | edge

    def quad(head):
        count = {0: 4, 16: 2}.get(head, 3)
        pltpu.make_async_remote_copy(
            src_ref=mem.at[head // 4, 0:count], dst_ref=mem.at[head // 4, 0:count], send_sem=msend,
            recv_sem=mrecv.at[head // 4], device_id=partner, device_id_type=MESH,
        ).wait_recv()
        total = part[place_of(head)].astype(F32)
        for slot in range(count):
            total += mem[head // 4, slot].astype(F32)
        return total

    def chain(step_at, hop):
        return pltpu.make_async_remote_copy(
            src_ref=cout.at[step_at], dst_ref=cin.at[step_at], send_sem=csend.at[step_at], recv_sem=crecv.at[step_at],
            device_id={"z": at(hop)}, device_id_type=MESH,
        )

    right = [chain(i, 4) for i in range(4)]
    left = [chain(4 + i, -4) for i in range(3)]
    for head in (16, 12, 20):
        members(head, late)
    cout[0] = quad(16).astype(BF16)
    right[0].start()
    cout[4] = quad(20).astype(BF16)
    left[0].start()
    for head in (8, 24):
        members(head, late)
    total = quad(12)
    right[0].wait_recv()
    cout[1] = (total + cin[0].astype(F32)).astype(BF16)
    right[1].start()
    total = quad(24)
    left[0].wait_recv()
    cout[5] = (total + cin[4].astype(F32)).astype(BF16)
    left[1].start()
    for head in (4, 28):
        members(head, late)
    total = quad(8)
    right[1].wait_recv()
    cout[2] = (total + cin[1].astype(F32)).astype(BF16)
    right[2].start()
    total = quad(28)
    left[1].wait_recv()
    cout[6] = (total + cin[5].astype(F32)).astype(BF16)
    left[2].start()
    members(0, late)
    total = quad(4)
    right[2].wait_recv()
    cout[3] = (total + cin[2].astype(F32)).astype(BF16)
    right[3].start()
    total = quad(0)
    left[2].wait_recv()
    total += cin[6].astype(F32)
    right[3].wait_recv()
    total += cin[3].astype(F32)
    owned = total.astype(BF16)

    urow = iota((8 * CB, 16), 0)
    ucol = iota((8 * CB, 16), 1)
    ublk, uj = urow // 8, lax.rem(urow, 8) - 3
    unpack = one_hot((ucol == uj * CB + ublk) & (uj >= 0) & (uj < 3))
    wide_rows = dot(unpack, owned)
    fresh = jnp.concatenate([wide_rows[cb * 8 : (cb + 1) * 8] for cb in range(CB)], axis=1)
    span = fresh[:, :2304] + context
    gate = pltpu.roll(fresh[:, 2304:4352], 5, 0)

    conv = span * taps[0:1]
    for k in range(1, 4):
        conv += pltpu.roll(span, 8 - k, 0) * taps[k : k + 1]
    live = iota(conv.shape, 0) < 3
    act = jnp.where(live, silu(conv), 0.0)
    x = act[:, :2048]
    inject = act[:, 2048:2176]
    readout = act[:, 2176:2304]
    x1 = pltpu.roll(x, 1, 0)
    x2 = pltpu.roll(x, 2, 0)
    i1 = pltpu.roll(inject, 1, 0)
    i2 = pltpu.roll(inject, 2, 0)

    outs = []
    for g in range(2):
        at_g = slice(g * 1024, (g + 1) * 1024)
        half = slice(g * 64, (g + 1) * 64)
        rd = readout[:, half]
        r_hi = rd.astype(BF16)
        r_lo = (rd - r_hi.astype(F32)).astype(BF16)
        both = jnp.concatenate([r_hi, r_hi], axis=1)
        low = jnp.concatenate([r_lo, jnp.zeros_like(r_lo)], axis=1)
        s_part = s0cat[at_g, :]
        first = dot_nt(both, s_part) + dot_nt(low, s_part)
        d0 = jnp.sum(rd * inject[:, half], axis=1, keepdims=True)
        d1 = jnp.sum(rd * i1[:, half], axis=1, keepdims=True)
        d2 = jnp.sum(rd * i2[:, half], axis=1, keepdims=True)
        response = (
            carry_w[:, at_g] * first
            + mix0[:, at_g] * x[:, at_g] * d0
            + mix1[:, at_g] * x1[:, at_g] * d1
            + mix2[:, at_g] * x2[:, at_g] * d2
            + direct[:, at_g] * x[:, at_g]
        )
        gated = jnp.where(live[:, :1024], response * silu(gate[:, at_g]), 0.0)
        norm = lax.rsqrt(jnp.sum(gated * gated, axis=1, keepdims=True) * (1.0 / 1024) + EPS)
        outs.append(gated * norm * gns[:, at_g])
    gated = jnp.concatenate(outs, axis=1)

    stack = jnp.concatenate([gated[:, cb * GBLK : (cb + 1) * GBLK] for cb in range(CB)], axis=0).astype(BF16)
    prow = iota((16, 8 * CB), 0)
    pcol = iota((16, 8 * CB), 1)
    packed = dot(one_hot(prow == lax.rem(pcol, 8) * CB + pcol // 8), stack)
    rest = gated[:, CB * GBLK :]
    last = jnp.concatenate([rest[j : j + 1] for j in range(3)], axis=1)
    packed = jnp.where(iota((16, GBLK), 0) == 15, jnp.broadcast_to(last, (16, GBLK)), packed)
    gown[...] = packed.astype(BF16)
    gath[z] = packed.astype(BF16)

    def share(src_ref, slot, hop, recv):
        pltpu.make_async_remote_copy(
            src_ref=src_ref, dst_ref=gath.at[slot], send_sem=gsend, recv_sem=recv, device_id={"z": at(hop)},
            device_id_type=MESH,
        ).start()

    for k in (4, 3, 5, 2, 6, 1, 7):
        share(gown, z, 4 * k, grecv.at[k])
    for hop in (-2, -1, 1, 2):
        share(gown, z, hop, nrecv)

    for g in range(2):
        at_g = slice(g * 1024, (g + 1) * 1024)
        half = slice(g * 64, (g + 1) * 64)
        b8 = inject[:, half]
        b_hi = b8.astype(BF16).astype(F32)
        b_lo = b8 - b_hi
        rhs = jnp.concatenate([b_hi, b_lo, b_hi], axis=0).astype(BF16)
        live0 = iota((8, 1024), 0)
        for j in range(3):
            coef = jnp.zeros((8, 1024), F32)
            for i in range(j + 1):
                mix = (mix0, mix1, mix2)[j - i]
                coef = jnp.where(live0 == i, mix[j : j + 1, at_g], coef)
            a8 = coef * x[:, at_g]
            a_hi = a8.astype(BF16).astype(F32)
            a_lo = a8 - a_hi
            lhs = jnp.concatenate([a_hi, a_hi, a_lo], axis=0).astype(BF16)
            snew[j, at_g, :] += dot_tn(lhs, rhs)
    groups = [
        jnp.concatenate(
            [
                span[:, g * 1024 : (g + 1) * 1024],
                span[:, 2048 + g * 64 : 2048 + (g + 1) * 64],
                span[:, 2176 + g * 64 : 2176 + (g + 1) * 64],
            ],
            axis=1,
        )
        for g in range(2)
    ]
    for i in range(6):
        tail_o[i] = jnp.concatenate([groups[0][i : i + 1], groups[1][i : i + 1]], axis=0).astype(BF16)

    for k in (1, 7, 2, 6, 3, 5, 4):
        slot = at(-4 * k)
        pltpu.make_async_remote_copy(
            src_ref=gown, dst_ref=gath.at[slot], send_sem=gsend, recv_sem=grecv.at[k], device_id=partner, device_id_type=MESH
        ).wait_recv()
        for hop in (-1, 1) + ((2,) if k < 4 else (-2,) if k > 4 else ()):
            share(gath.at[slot], slot, hop, nrecv)
    pltpu.make_async_remote_copy(
        src_ref=gath.at[0:24], dst_ref=gath.at[0:24], send_sem=gsend, recv_sem=nrecv, device_id=partner, device_id_type=MESH
    ).wait_recv()

    srow = iota((32 * CB, 128), 0)
    scol = iota((32 * CB, 128), 1)
    m, scb = lax.rem(srow, 32), srow // 32
    select = one_hot((m // 4 == scol // 16) & (lax.rem(scol, 16) == lax.rem(m, 4) * CB + scb) & (lax.rem(m, 4) < 3))
    m2 = iota((32, 128), 0)
    c2 = iota((32, 128), 1)
    pick = [one_hot((m2 // 4 == c2 // 16) & (lax.rem(c2, 16) == 15) & (lax.rem(m2, 4) == j)) for j in range(3)]
    inputs = []
    for tb in range(4):
        block = gath[tb * 8 : (tb + 1) * 8].reshape(128, GBLK)
        y = dot(select, block)
        tail = sum(dot(pick[j], block[:, j * 128 : (j + 1) * 128]) for j in range(3))
        inputs.append(jnp.concatenate([y[cb * 32 : (cb + 1) * 32] for cb in range(CB)] + [tail], axis=1).astype(BF16))
    full = jnp.concatenate(inputs, axis=0)
    own_cols = dot_nt(full, wo[...]).astype(BF16)
    partner_cols = dot_nt(full, wop[...]).astype(BF16)
    for tb in range(4):
        fst[0, tb] = own_cols[tb * 32 : (tb + 1) * 32]
        fst[1, tb] = partner_cols[tb * 32 : (tb + 1) * 32]

    finals = []
    for i, (dc, dt) in enumerate(others):
        to = lax.rem(t + dt, n_tp)
        finals.append(
            pltpu.make_async_remote_copy(
                src_ref=fst.at[dc, to], dst_ref=fin.at[c, t], send_sem=fsend.at[i], recv_sem=frecv.at[i],
                device_id={"c": lax.rem(c + dc, 2), "tp": to}, device_id_type=MESH,
            )
        )
    for cp in finals:
        cp.start()
    fin[c, t] = fst[0, t]
    for cp in finals:
        cp.wait_recv()
    totals = []
    for k in range(2):
        total = fin[k, 0].astype(F32)
        for i in range(1, 4):
            total += fin[k, i].astype(F32)
        totals.append(total.astype(BF16))
    trow = iota((48, 32), 0)
    tcol = iota((48, 32), 1)
    want = 4 * (lax.rem(trow, 16) // 2) + trow // 16
    arranged = sum(dot(one_hot((lax.rem(trow, 2) == k) & (tcol == want)), totals[k]) for k in range(2))
    for j in range(3):
        mixed_o[j] = arranged[j * 16 : (j + 1) * 16].astype(BF16)

    @pl.when(o + 8 < LAST)
    def _():
        def left_right(slot, _):
            copy_slice(rel0.at[slot], rel0.at[slot], r0send.at[slot], arecv.at[0], o + 8).wait_send()
            return 0

        lax.fori_loop(jnp.maximum(8 - o, 0), 8, left_right, 0)

    @pl.when(o + LAST < NZ)
    def _():
        def left_wrap(slot, _):
            @pl.when(slot != o)
            def _():
                copy_slice(rel2.at[slot], rel2.at[slot], r2send.at[slot], arecv.at[0], o + LAST).wait_send()

            return 0

        lax.fori_loop(0, CLOSE, left_wrap, 0)

    @pl.when(o + 24 < LAST)
    def _():
        def left_left(slot, _):
            copy_slice(rel1.at[slot], rel1.at[slot], r1send.at[slot], arecv.at[0], o + 24).wait_send()
            return 0

        lax.fori_loop(0, 7, left_left, 0)

    for cp in shares:
        cp.wait_send()
    for cp in right + left:
        cp.wait_send()
    for cp in finals:
        cp.wait_send()
    for ref, count, sem in ((xs, NZ - 1, asend), (part, 24, msend), (gath, NZ - 1, gsend)):
        pltpu.make_async_remote_copy(
            src_ref=ref.at[0:count], dst_ref=ref.at[0:count], send_sem=sem, recv_sem=arecv.at[0], device_id=partner,
            device_id_type=MESH,
        ).wait_send()


def store(mixed, states, tail, mixed_o, states_o, tail_o, sem):
    copies = [
        pltpu.make_async_copy(src, dst, sem.at[i])
        for i, (src, dst) in enumerate(((states, states_o), (tail, tail_o), (mixed, mixed_o)))
    ]
    for cp in copies:
        cp.start()
    for cp in copies:
        cp.wait()


def local(
    tokens,
    input_norm_scale,
    head_input_matrix,
    output_gate_matrix,
    group_input_matrix,
    group_readout_matrix,
    step_size_matrix,
    step_size_bias,
    log_decay_rate,
    direct_path_weight,
    convolution_tap_weight,
    convolution_history_rows,
    per_proposal_states,
    accepted,
    proposal_extra_decay,
    group_norm_scale,
    output_projection_matrix,
):
    width = tokens.shape[2]
    heads = step_size_bias.shape[0]
    channels = heads * 64
    dma = pltpu.SemaphoreType.DMA
    any_space = pl.BlockSpec(memory_space=pl.ANY)
    vmem = pl.BlockSpec(memory_space=pltpu.VMEM)
    mixed, states, tail = pl.pallas_call(
        kernel,
        name="mixer",
        out_shape=(
            pltpu.VMEM((3, 16, 64), BF16),
            pltpu.VMEM((3, channels, 64), F32),
            pltpu.VMEM((6, 2, 1152), BF16),
        ),
        in_specs=[any_space] * 17,
        out_specs=(vmem, vmem, vmem),
        scratch_shapes=[
            pltpu.VMEM((3, width), BF16),
            pltpu.VMEM((1, width), F32),
            pltpu.VMEM((heads, width), BF16),
            pltpu.VMEM((1, heads), F32),
            pltpu.VMEM((1, heads), F32),
            pltpu.VMEM((1, heads), F32),
            pltpu.VMEM((4, 2, 1152), BF16),
            pltpu.VMEM((6, 2, 1152), BF16),
            pltpu.VMEM((3, channels, 64), F32),
            pltpu.VMEM((3, 1, heads), F32),
            pltpu.VMEM((1, channels), F32),
            pltpu.VMEM((64, channels), BF16),
            pltpu.VMEM((64, channels), BF16),
            pltpu.VMEM((CB * 128, BLK), BF16),
            pltpu.VMEM((NZ, 4, 128), BF16),
            pltpu.VMEM((NZ, 4, 128), BF16),
            pltpu.VMEM((NZ, 16, BLK), BF16),
            pltpu.VMEM((8, 4, 16, BLK), BF16),
            pltpu.VMEM((7, 16, BLK), BF16),
            pltpu.VMEM((7, 16, BLK), BF16),
            pltpu.VMEM((NZ, 16, GBLK), BF16),
            pltpu.VMEM((16, GBLK), BF16),
            pltpu.VMEM((2, 4, 32, 64), BF16),
            pltpu.VMEM((2, 4, 32, 64), BF16),
            pltpu.VMEM((channels, 128), BF16),
            dma((13 + len(PIECES),)),
            dma((len(PIECES) + 1,)),
            dma((len(PIECES) + 1,)),
            dma,
            dma((3,)),
            dma,
            dma((8,)),
            dma((7,)),
            dma((7,)),
            dma,
            dma((8,)),
            dma,
            dma((7,)),
            dma((7,)),
            pltpu.VMEM((8, 4, 128), BF16),
            pltpu.VMEM((7, 4, 128), BF16),
            dma((8,)),
            dma((8,)),
            dma((7,)),
            dma((7,)),
            pltpu.SemaphoreType.REGULAR((NZ,)),
            pltpu.SMEM((1,), jnp.int32),
            pltpu.VMEM((CLOSE, 4, 128), BF16),
            dma((CLOSE,)),
            dma((CLOSE,)),
        ],
        compiler_params=pltpu.CompilerParams(
            collective_id=0, has_side_effects=True, vmem_limit_bytes=56 * 1024 * 1024
        ),
    )(
        tokens,
        input_norm_scale.reshape(1, width),
        head_input_matrix,
        output_gate_matrix,
        group_input_matrix,
        group_readout_matrix,
        step_size_matrix.T,
        step_size_bias.reshape(1, heads),
        log_decay_rate.reshape(1, heads),
        direct_path_weight.reshape(1, heads),
        convolution_tap_weight,
        convolution_history_rows,
        per_proposal_states.reshape(3, channels, 64),
        accepted,
        proposal_extra_decay.transpose(1, 0, 2),
        group_norm_scale.reshape(1, channels),
        output_projection_matrix.T,
    )
    mixed, states, tail = pl.pallas_call(
        store,
        name="store",
        out_shape=(
            jax.ShapeDtypeStruct((3, 16, 64), BF16),
            jax.ShapeDtypeStruct((3, channels, 64), F32),
            jax.ShapeDtypeStruct((6, 2, 1152), BF16),
        ),
        in_specs=[pl.BlockSpec(memory_space=pltpu.VMEM)] * 3,
        out_specs=(any_space,) * 3,
        scratch_shapes=[dma((3,))],
    )(*(pltpu.with_memory_space_constraint(v, pltpu.VMEM) for v in (mixed, states, tail)))
    mixed = mixed.transpose(1, 0, 2)
    states = states.reshape(1, 3, heads, 64, 64)
    tail = tail[None]
    return mixed, states, tail


def solution(mesh):
    ring = mesh.shape["kv"] // 2
    assert ring == NZ and mesh.shape["tp"] == 4
    finer = Mesh(
        mesh.devices.reshape(mesh.shape["grp"], ring, 2, mesh.shape["tp"]),
        ("grp", "z", "c", "tp"),
    )
    return jax.shard_map(
        local,
        mesh=finer,
        in_specs=(
            P(GRP_KV, None, None),
            P(),
            P(KV, "tp"),
            P(KV, "tp"),
            P(KV, "tp"),
            P(KV, "tp"),
            P(None, "tp"),
            P("tp"),
            P("tp"),
            P("tp"),
            P(None, "tp", None),
            P(GRP_KV, None, "tp", None),
            P(GRP_KV, None, "tp", None, None),
            P(GRP_KV),
            P(GRP_KV, None, "tp"),
            P("tp"),
            P("tp", KV),
        ),
        out_specs=(
            P(("grp", "tp"), None, KV),
            P(GRP_KV, None, "tp", None, None),
            P(GRP_KV, None, "tp", None),
        ),
        check_vma=False,
    )
```

```python
import functools

import jax
import jax.numpy as jnp
from jax import lax
from jax.experimental import pallas as pl
from jax.experimental.pallas import tpu as pltpu
from jax.sharding import Mesh
from jax.sharding import PartitionSpec as P

MESH = pl.DeviceIdType.MESH
EPS = 1e-06
F32 = jnp.float32
BF16 = jnp.bfloat16

KV = ("z", "c")
GRP_KV = ("grp", "z", "c")

STAGES = (0, 16, 24, 32)
LAST = 28
CLOSE = 26
FIRST = 8
NZ = 32
BLK = 896
CB = 5
GBLK = 384


def iota(shape, dim):
    return lax.broadcasted_iota(jnp.int32, shape, dim)


def split3(v):
    hi = v.astype(BF16)
    rest = v - hi.astype(F32)
    mid = rest.astype(BF16)
    lo = (rest - mid.astype(F32)).astype(BF16)
    return hi, mid, lo


def dot(a, b):
    return jnp.dot(a, b, preferred_element_type=F32)


def dot_nt(a, b):
    return lax.dot_general(a, b, (((1,), (1,)), ((), ())), preferred_element_type=F32)


def dot_tn(a, b):
    return lax.dot_general(a, b, (((0,), (0,)), ((), ())), preferred_element_type=F32)


def silu(v):
    return v / (1.0 + jnp.exp(-v))


def one_hot(cond):
    return jnp.where(cond, 1.0, 0.0).astype(BF16)


PIECES = (
    (0, 0, 896, 0, 0),
    (0, 896, 896, 1, 0),
    (0, 1792, 256, 2, 0),
    (2, 0, 128, 2, 256),
    (3, 0, 128, 2, 384),
    (1, 0, 384, 2, 512),
    (1, 384, 896, 3, 0),
    (1, 1280, 768, 4, 0),
)


def kernel(
    tok_h, ins_h, wh_h, wg_h, wi_h, wr_h, ws_h, bias_h, ldr_h, dpw_h, tap_h, hist_h, st_h, acc_h, ped_h, gns_h, wo_h,
    mixed_o, snew, tail_o,
    tok, ins, ws, bias, ldr, dpw, tap, hist, st, ped, gns, wo, wop,
    w2, nst, xs, part, mem, cout, cin, gath, gown, fin, fst, s0cat,
    lsem, wsend, wrecv, asend, arecv, msend, mrecv, csend, crecv, gsend, grecv, nrecv, fsend, frecv, rel0, rel1, r0send, r0recv, r1send, r1recv, may, acc_s, rel2, r2send, r2recv,
):
    z = lax.axis_index("z")
    c = lax.axis_index("c")
    t = lax.axis_index("tp")
    n_tp = lax.axis_size("tp")

    o = lax.rem(z + NZ - 1, NZ)

    def at(offset):
        return lax.rem(z + (offset + NZ) % NZ, NZ)

    def place_of(offset):
        return lax.rem(o + (offset + NZ) % NZ, NZ)

    def chip(place):
        return lax.rem(place + 1, NZ)

    def stage_of(place):
        return jnp.where(place < STAGES[1], 0, jnp.where(place < STAGES[2], 1, 2))

    pairs = [
        (tok_h.at[0], tok), (ins_h, ins), (ws_h, ws), (bias_h, bias), (ldr_h, ldr), (dpw_h, dpw), (tap_h, tap),
        (hist_h.at[0], hist), (ped_h, ped), (gns_h, gns), (st_h, st), (wo_h, wo), (acc_h, acc_s),
    ]
    loads = [pltpu.make_async_copy(src, dst, lsem.at[i]) for i, (src, dst) in enumerate(pairs)]
    sources = (wh_h, wg_h, wi_h, wr_h)
    mine = pl.multiple_of(c * 64, 64)
    for i, (source, first, count, row, lane) in enumerate(PIECES):
        loads.append(
            pltpu.make_async_copy(
                sources[source].at[:, first : first + count],
                w2.at[pl.ds(pl.multiple_of(row * 128 + mine, 64), 64), lane : lane + count],
                lsem.at[len(pairs) + i],
            )
        )
    for cp in loads:
        cp.start()

    barrier = pltpu.get_barrier_semaphore()

    def greet(to, _):
        pl.semaphore_signal(barrier, inc=1, device_id={"z": chip(to)}, device_id_type=MESH)
        return 0

    lax.fori_loop(o + 1, NZ, greet, 0)
    others = [(dc, dt) for dc in range(2) for dt in range(n_tp) if (dc, dt) != (0, 0)]
    for dc, dt in others:
        pl.semaphore_signal(
            barrier, inc=1, device_id={"c": lax.rem(c + dc, 2), "tp": lax.rem(t + dt, n_tp)}, device_id_type=MESH
        )

    pl.semaphore_wait(barrier, o + len(others))

    def tell(k, _):
        to = chip(o - k)

        usual = (k <= 8) | (k >= 24) | ((k >= 17) & (o < 24))
        last = (k == LAST) | (k <= o - CLOSE)

        @pl.when(((o < LAST) & usual) | ((o >= LAST) & last))
        def _():
            pl.semaphore_signal(may.at[o], inc=1, device_id={"z": to}, device_id_type=MESH)

        return 0

    lax.fori_loop(1, o + 1, tell, 0)

    loads[0].wait()
    loads[1].wait()
    wide = tok[...].astype(F32)
    scale = lax.rsqrt(jnp.sum(wide * wide, axis=-1, keepdims=True) * (1.0 / wide.shape[1]) + EPS)
    normed = (wide * scale * ins[...]).astype(BF16)
    padded = jnp.concatenate([normed.astype(F32), jnp.zeros((1, normed.shape[1]), F32)], axis=0).astype(BF16)
    for k in range(NZ):
        nst[k] = padded[:, k * 128 : (k + 1) * 128]

    def copy_slice(src_ref, dst_ref, send_sem, recv_sem, to):
        return pltpu.make_async_remote_copy(
            src_ref=src_ref, dst_ref=dst_ref, send_sem=send_sem, recv_sem=recv_sem, device_id={"z": chip(to)},
            device_id_type=MESH,
        )

    def direct_slice(to):
        copy_slice(nst.at[chip(to)], xs.at[o], asend, arecv.at[stage_of(o)], to).start()

    def send_back(to, _):
        direct_slice(to)
        return 0

    lax.fori_loop(0, o, send_back, 0)

    def send_by_first(to, _):
        relay = to - 24
        copy_slice(nst.at[chip(to)], rel1.at[o - relay - 1], asend, r1recv.at[o - relay - 1], relay).start()
        return 0

    lax.fori_loop(jnp.maximum(o + 17, 24), jnp.minimum(o + 24, LAST), send_by_first, 0)

    def send_by_wrap(relay, _):
        copy_slice(nst.at[chip(relay + LAST)], rel2.at[o], asend, r2recv.at[o], relay).start()
        return 0

    @pl.when(o < CLOSE)
    def _():
        lax.fori_loop(0, jnp.minimum(o, NZ - LAST), send_by_wrap, 0)

    xs[o] = nst[z]

    partner = {"c": 1 - c}
    shares = []
    for i, (source, first, count, row, lane) in enumerate(PIECES):
        shares.append(
            pltpu.make_async_remote_copy(
                src_ref=sources[source].at[:, first : first + count],
                dst_ref=w2.at[pl.ds(pl.multiple_of(row * 128 + mine, 64), 64), lane : lane + count],
                send_sem=wsend.at[i], recv_sem=wrecv.at[i], device_id=partner, device_id_type=MESH,
            )
        )
    shares.append(
        pltpu.make_async_remote_copy(
            src_ref=wo_h, dst_ref=wop, send_sem=wsend.at[len(PIECES)], recv_sem=wrecv.at[len(PIECES)],
            device_id=partner, device_id_type=MESH,
        )
    )
    for cp in shares:
        cp.start()

    for cp in loads[2:]:
        cp.wait()
    w2[4 * 128 :, 768:] = jnp.zeros((128, 128), BF16)
    step_raw = dot_nt(normed, ws[...])
    raw = step_raw + bias[...]
    step = jnp.maximum(raw, 0.0) + jnp.log1p(jnp.exp(-jnp.abs(raw)))
    decay = jnp.exp(ldr[...]) * step
    cum0 = ped[0] - decay[0:1]
    cum1 = cum0 + (ped[1] - decay[1:2])
    cum2 = cum1 + (ped[2] - decay[2:3])
    none = jnp.zeros_like(cum0)
    zeros5 = jnp.zeros((5, cum0.shape[1]), F32)

    def rows(a, b, d):
        return jnp.concatenate([a, b, d, zeros5], axis=0)

    per_head = jnp.concatenate(
        [
            rows(jnp.exp(cum0), jnp.exp(cum1), jnp.exp(cum2)),
            rows(step[0:1], step[1:2], step[2:3]),
            rows(none, jnp.exp(cum1 - cum0) * step[0:1], jnp.exp(cum2 - cum1) * step[1:2]),
            rows(none, none, jnp.exp(cum2 - cum0) * step[0:1]),
            rows(dpw[...], dpw[...], dpw[...]),
        ],
        axis=0,
    )
    heads = per_head.shape[1]
    lanes = heads * 64
    to_head = iota((heads, lanes), 1) - iota((heads, lanes), 0) * 64
    expand = one_hot((to_head >= 0) & (to_head < 64))
    hi, mid, lo = split3(per_head)
    wide_heads = dot(hi, expand) + dot(mid, expand) + dot(lo, expand)
    carry_w, mix0, mix1, mix2, direct = (wide_heads[i * 8 : (i + 1) * 8] for i in range(5))

    start = jnp.clip(acc_s[0] - 1, 0, 2)
    ones3 = jnp.ones((3, 64), BF16)
    for g in range(2):
        at_g = slice(g * 1024, (g + 1) * 1024)
        s0 = st[start, at_g, :]
        s_hi = s0.astype(BF16)
        s_lo = (s0 - s_hi.astype(F32)).astype(BF16)
        s0cat[at_g, :] = jnp.concatenate([s_hi, s_lo], axis=1)
        for j in range(3):
            line = carry_w[j : j + 1, at_g]
            l_hi, l_mid, l_lo = split3(line)
            stack = jnp.concatenate([l_hi.astype(F32), l_mid.astype(F32), l_lo.astype(F32)], axis=0).astype(BF16)
            snew[j, at_g, :] = dot_tn(stack, ones3) * s0

    def in_order(v):
        a, b = v[:, 0, :], v[:, 1, :]
        return jnp.concatenate(
            [a[:, :1024], b[:, :1024], a[:, 1024:1088], b[:, 1024:1088], a[:, 1088:], b[:, 1088:]], axis=1
        )

    kept = in_order(hist[...].astype(F32))
    taps = in_order(tap[...].astype(F32))
    accepted = acc_s[0]
    context = jnp.where(accepted == 1, kept[1:4], jnp.where(accepted == 2, kept[2:5], kept[3:6]))
    context = jnp.concatenate([context, jnp.zeros((5, context.shape[1]), F32)], axis=0)

    to_row = iota((128, 32), 0)
    from_row = iota((128, 32), 1)
    packed_row = lax.rem(to_row, 16)
    spread = one_hot((to_row // 16 == from_row // 4) & (packed_row // CB == lax.rem(from_row, 4)) & (packed_row < 3 * CB))

    def member(delta, hop, head, slot, when):
        dest = place_of(delta)

        @pl.when(when(stage_of(dest), o + hop < 0))
        def _():
            pltpu.make_async_remote_copy(
                src_ref=part.at[dest], dst_ref=mem.at[head // 4, slot], send_sem=msend, recv_sem=mrecv.at[head // 4],
                device_id={"z": at(hop)}, device_id_type=MESH,
            ).start()

    def members(head, when):
        member((head + 1) % NZ, 1, head, 0, when)
        member((head - 1) % NZ, -1, head, 1, when)
        if head < 16:
            member(head + 2, 2, head, 2, when)
        if head > 16:
            member(head - 2, -2, head, 2, when)
        if head == 0:
            member(NZ - 2, -2, head, 3, when)

    def arrived(stage):
        first, last = STAGES[stage], STAGES[stage + 1]

        def wait(count):
            pltpu.make_async_remote_copy(
                src_ref=xs.at[0:count], dst_ref=xs.at[0:count], send_sem=asend, recv_sem=arecv.at[stage],
                device_id=partner, device_id_type=MESH,
            ).wait_recv()

        @pl.when(stage_of(o) == stage)
        def _():
            wait(last - first - 1)

        @pl.when(stage_of(o) != stage)
        def _():
            wait(last - first)

    def multiply(stage):
        first, last = STAGES[stage], STAGES[stage + 1]
        rows = (last - first) * 16
        x_rows = jnp.concatenate([xs[k].astype(F32) for k in range(first, last)], axis=0).astype(BF16)
        x_all = jnp.concatenate([dot(spread, x_rows[i : i + 32]) for i in range(0, x_rows.shape[0], 32)], axis=0)
        x_all = x_all.astype(BF16)
        block_of = lax.rem(lax.rem(iota((rows, 128), 0), 16), CB)
        zero = jnp.zeros_like(x_all)
        stacked = jnp.concatenate([jnp.where(block_of == cb, x_all, zero) for cb in range(CB)], axis=1)
        for n0, n1 in ((0, 256), (256, 512), (512, 768), (768, 896)):
            part[first:last, :, n0:n1] = dot(stacked, w2[:, n0:n1]).astype(BF16).reshape(last - first, 16, n1 - n0)

    def send_near(to, _):
        pl.semaphore_wait(may.at[to], 1)
        direct_slice(to)

        @pl.when(to + 8 < LAST)
        def _():
            slot = o - to + 8
            copy_slice(nst.at[chip(to + 8)], rel0.at[slot], asend, r0recv.at[slot], to).start()

        return 0

    lax.fori_loop(o + 1, jnp.minimum(o + 9, jnp.where(o < CLOSE, LAST, NZ)), send_near, 0)
    lax.fori_loop(o + 1, NZ - LAST, send_by_wrap, 0)

    def pass_on(rel, slot, source, sems, recv, to):
        copy_slice(rel.at[slot], rel.at[slot], asend, recv.at[slot], to).wait_recv()
        copy_slice(rel.at[slot], xs.at[source], sems.at[slot], arecv.at[stage_of(source)], to).start()

    @pl.when(o + 8 < LAST)
    def _():
        def pass_right(slot, _):
            pass_on(rel0, slot, o - 8 + slot, r0send, r0recv, o + 8)
            return 0

        lax.fori_loop(jnp.maximum(8 - o, 0), 8, pass_right, 0)

    def send_far(to, _):
        pl.semaphore_wait(may.at[to], 1)
        direct_slice(to)
        return 0

    lax.fori_loop(o + 17, STAGES[2], send_far, 0)

    for cp in shares:
        cp.wait_recv()
    arrived(0)
    multiply(0)
    for head in (16, 12, 20, 8, 24, 4, 28, 0):
        members(head, lambda stage, edge: (o < STAGES[2]) & (stage == 0) & ~edge)

    @pl.when(o + 24 < LAST)
    def _():
        send_far(o + 24, 0)

        def pass_left(slot, _):
            pass_on(rel1, slot, o + 1 + slot, r1send, r1recv, o + 24)
            return 0

        lax.fori_loop(0, 7, pass_left, 0)

    lax.fori_loop(o + 25, LAST, send_far, 0)

    @pl.when(o + LAST < NZ)
    def _():
        send_far(o + LAST, 0)

        def pass_wrap(slot, _):
            @pl.when(slot != o)
            def _():
                pass_on(rel2, slot, slot, r2send, r2recv, o + LAST)

            return 0

        lax.fori_loop(0, CLOSE, pass_wrap, 0)


    arrived(1)
    multiply(1)
    for head in (16, 12, 20, 8, 24, 4, 28, 0):
        members(head, lambda stage, edge: (o < STAGES[2]) & (stage == 1) & ~edge)

    arrived(2)
    multiply(2)

    def late(stage, edge):
        return (o >= STAGES[2]) | (stage == 2) | edge

    def quad(head):
        count = {0: 4, 16: 2}.get(head, 3)
        pltpu.make_async_remote_copy(
            src_ref=mem.at[head // 4, 0:count], dst_ref=mem.at[head // 4, 0:count], send_sem=msend,
            recv_sem=mrecv.at[head // 4], device_id=partner, device_id_type=MESH,
        ).wait_recv()
        total = part[place_of(head)].astype(F32)
        for slot in range(count):
            total += mem[head // 4, slot].astype(F32)
        return total

    def chain(step_at, hop):
        return pltpu.make_async_remote_copy(
            src_ref=cout.at[step_at], dst_ref=cin.at[step_at], send_sem=csend.at[step_at], recv_sem=crecv.at[step_at],
            device_id={"z": at(hop)}, device_id_type=MESH,
        )

    right = [chain(i, 4) for i in range(4)]
    left = [chain(4 + i, -4) for i in range(3)]
    for head in (16, 12, 20):
        members(head, late)
    cout[0] = quad(16).astype(BF16)
    right[0].start()
    cout[4] = quad(20).astype(BF16)
    left[0].start()
    for head in (8, 24):
        members(head, late)
    total = quad(12)
    right[0].wait_recv()
    cout[1] = (total + cin[0].astype(F32)).astype(BF16)
    right[1].start()
    total = quad(24)
    left[0].wait_recv()
    cout[5] = (total + cin[4].astype(F32)).astype(BF16)
    left[1].start()
    for head in (4, 28):
        members(head, late)
    total = quad(8)
    right[1].wait_recv()
    cout[2] = (total + cin[1].astype(F32)).astype(BF16)
    right[2].start()
    total = quad(28)
    left[1].wait_recv()
    cout[6] = (total + cin[5].astype(F32)).astype(BF16)
    left[2].start()
    members(0, late)
    total = quad(4)
    right[2].wait_recv()
    cout[3] = (total + cin[2].astype(F32)).astype(BF16)
    right[3].start()
    total = quad(0)
    left[2].wait_recv()
    total += cin[6].astype(F32)
    right[3].wait_recv()
    total += cin[3].astype(F32)
    owned = total.astype(BF16)

    urow = iota((8 * CB, 16), 0)
    ucol = iota((8 * CB, 16), 1)
    ublk, uj = urow // 8, lax.rem(urow, 8) - 3
    unpack = one_hot((ucol == uj * CB + ublk) & (uj >= 0) & (uj < 3))
    wide_rows = dot(unpack, owned)
    fresh = jnp.concatenate([wide_rows[cb * 8 : (cb + 1) * 8] for cb in range(CB)], axis=1)
    span = fresh[:, :2304] + context
    gate = pltpu.roll(fresh[:, 2304:4352], 5, 0)

    conv = span * taps[0:1]
    for k in range(1, 4):
        conv += pltpu.roll(span, 8 - k, 0) * taps[k : k + 1]
    live = iota(conv.shape, 0) < 3
    act = jnp.where(live, silu(conv), 0.0)
    x = act[:, :2048]
    inject = act[:, 2048:2176]
    readout = act[:, 2176:2304]
    x1 = pltpu.roll(x, 1, 0)
    x2 = pltpu.roll(x, 2, 0)
    i1 = pltpu.roll(inject, 1, 0)
    i2 = pltpu.roll(inject, 2, 0)

    outs = []
    for g in range(2):
        at_g = slice(g * 1024, (g + 1) * 1024)
        half = slice(g * 64, (g + 1) * 64)
        rd = readout[:, half]
        r_hi = rd.astype(BF16)
        r_lo = (rd - r_hi.astype(F32)).astype(BF16)
        both = jnp.concatenate([r_hi, r_hi], axis=1)
        low = jnp.concatenate([r_lo, jnp.zeros_like(r_lo)], axis=1)
        s_part = s0cat[at_g, :]
        first = dot_nt(both, s_part) + dot_nt(low, s_part)
        d0 = jnp.sum(rd * inject[:, half], axis=1, keepdims=True)
        d1 = jnp.sum(rd * i1[:, half], axis=1, keepdims=True)
        d2 = jnp.sum(rd * i2[:, half], axis=1, keepdims=True)
        response = (
            carry_w[:, at_g] * first
            + mix0[:, at_g] * x[:, at_g] * d0
            + mix1[:, at_g] * x1[:, at_g] * d1
            + mix2[:, at_g] * x2[:, at_g] * d2
            + direct[:, at_g] * x[:, at_g]
        )
        gated = jnp.where(live[:, :1024], response * silu(gate[:, at_g]), 0.0)
        norm = lax.rsqrt(jnp.sum(gated * gated, axis=1, keepdims=True) * (1.0 / 1024) + EPS)
        outs.append(gated * norm * gns[:, at_g])
    gated = jnp.concatenate(outs, axis=1)

    stack = jnp.concatenate([gated[:, cb * GBLK : (cb + 1) * GBLK] for cb in range(CB)], axis=0).astype(BF16)
    prow = iota((16, 8 * CB), 0)
    pcol = iota((16, 8 * CB), 1)
    packed = dot(one_hot(prow == lax.rem(pcol, 8) * CB + pcol // 8), stack)
    rest = gated[:, CB * GBLK :]
    last = jnp.concatenate([rest[j : j + 1] for j in range(3)], axis=1)
    packed = jnp.where(iota((16, GBLK), 0) == 15, jnp.broadcast_to(last, (16, GBLK)), packed)
    gown[...] = packed.astype(BF16)
    gath[z] = packed.astype(BF16)

    def share(src_ref, slot, hop, recv):
        pltpu.make_async_remote_copy(
            src_ref=src_ref, dst_ref=gath.at[slot], send_sem=gsend, recv_sem=recv, device_id={"z": at(hop)},
            device_id_type=MESH,
        ).start()

    for k in (4, 3, 5, 2, 6, 1, 7):
        share(gown, z, 4 * k, grecv.at[k])
    for hop in (-2, -1, 1, 2):
        share(gown, z, hop, nrecv)

    for g in range(2):
        at_g = slice(g * 1024, (g + 1) * 1024)
        half = slice(g * 64, (g + 1) * 64)
        b8 = inject[:, half]
        b_hi = b8.astype(BF16).astype(F32)
        b_lo = b8 - b_hi
        rhs = jnp.concatenate([b_hi, b_lo, b_hi], axis=0).astype(BF16)
        live0 = iota((8, 1024), 0)
        for j in range(3):
            coef = jnp.zeros((8, 1024), F32)
            for i in range(j + 1):
                mix = (mix0, mix1, mix2)[j - i]
                coef = jnp.where(live0 == i, mix[j : j + 1, at_g], coef)
            a8 = coef * x[:, at_g]
            a_hi = a8.astype(BF16).astype(F32)
            a_lo = a8 - a_hi
            lhs = jnp.concatenate([a_hi, a_hi, a_lo], axis=0).astype(BF16)
            snew[j, at_g, :] += dot_tn(lhs, rhs)
    groups = [
        jnp.concatenate(
            [
                span[:, g * 1024 : (g + 1) * 1024],
                span[:, 2048 + g * 64 : 2048 + (g + 1) * 64],
                span[:, 2176 + g * 64 : 2176 + (g + 1) * 64],
            ],
            axis=1,
        )
        for g in range(2)
    ]
    for i in range(6):
        tail_o[i] = jnp.concatenate([groups[0][i : i + 1], groups[1][i : i + 1]], axis=0).astype(BF16)

    @pl.when(o + 8 < LAST)
    def _():
        def left_right(slot, _):
            copy_slice(rel0.at[slot], rel0.at[slot], r0send.at[slot], arecv.at[0], o + 8).wait_send()
            return 0

        lax.fori_loop(jnp.maximum(8 - o, 0), 8, left_right, 0)

    @pl.when(o + LAST < NZ)
    def _():
        def left_wrap(slot, _):
            @pl.when(slot != o)
            def _():
                copy_slice(rel2.at[slot], rel2.at[slot], r2send.at[slot], arecv.at[0], o + LAST).wait_send()

            return 0

        lax.fori_loop(0, CLOSE, left_wrap, 0)

    @pl.when(o + 24 < LAST)
    def _():
        def left_left(slot, _):
            copy_slice(rel1.at[slot], rel1.at[slot], r1send.at[slot], arecv.at[0], o + 24).wait_send()
            return 0

        lax.fori_loop(0, 7, left_left, 0)

    for cp in shares:
        cp.wait_send()
    for cp in right + left:
        cp.wait_send()
    for ref, count, sem in ((xs, NZ - 1, asend), (part, 24, msend)):
        pltpu.make_async_remote_copy(
            src_ref=ref.at[0:count], dst_ref=ref.at[0:count], send_sem=sem, recv_sem=arecv.at[0], device_id=partner,
            device_id_type=MESH,
        ).wait_send()

    def pass_gated(i, _):
        source = lax.rem(FIRST + lax.rem(z, 4) + 4 * i, NZ)
        k = lax.rem(z - source + NZ, NZ) // 4

        @pl.when(source != z)
        def _():
            pltpu.make_async_remote_copy(
                src_ref=gown, dst_ref=gath.at[source], send_sem=gsend, recv_sem=grecv.at[k], device_id=partner,
                device_id_type=MESH,
            ).wait_recv()
            share(gath.at[source], source, -1, nrecv)
            share(gath.at[source], source, 1, nrecv)

            @pl.when(k < 4)
            def _():
                share(gath.at[source], source, 2, nrecv)

            @pl.when(k > 4)
            def _():
                share(gath.at[source], source, -2, nrecv)

        return 0

    lax.fori_loop(0, NZ // 4, pass_gated, 0)
    pltpu.make_async_remote_copy(
        src_ref=gath.at[0:24], dst_ref=gath.at[0:24], send_sem=gsend, recv_sem=nrecv, device_id=partner, device_id_type=MESH
    ).wait_recv()

    srow = iota((32 * CB, 128), 0)
    scol = iota((32 * CB, 128), 1)
    m, scb = lax.rem(srow, 32), srow // 32
    select = one_hot((m // 4 == scol // 16) & (lax.rem(scol, 16) == lax.rem(m, 4) * CB + scb) & (lax.rem(m, 4) < 3))
    m2 = iota((32, 128), 0)
    c2 = iota((32, 128), 1)
    pick = [one_hot((m2 // 4 == c2 // 16) & (lax.rem(c2, 16) == 15) & (lax.rem(m2, 4) == j)) for j in range(3)]
    inputs = []
    for tb in range(4):
        block = gath[tb * 8 : (tb + 1) * 8].reshape(128, GBLK)
        y = dot(select, block)
        tail = sum(dot(pick[j], block[:, j * 128 : (j + 1) * 128]) for j in range(3))
        inputs.append(jnp.concatenate([y[cb * 32 : (cb + 1) * 32] for cb in range(CB)] + [tail], axis=1).astype(BF16))
    full = jnp.concatenate(inputs, axis=0)
    own_cols = dot_nt(full, wo[...]).astype(BF16)
    partner_cols = dot_nt(full, wop[...]).astype(BF16)
    for tb in range(4):
        fst[0, tb] = own_cols[tb * 32 : (tb + 1) * 32]
        fst[1, tb] = partner_cols[tb * 32 : (tb + 1) * 32]

    finals = []
    for i, (dc, dt) in enumerate(others):
        to = lax.rem(t + dt, n_tp)
        finals.append(
            pltpu.make_async_remote_copy(
                src_ref=fst.at[dc, to], dst_ref=fin.at[c, t], send_sem=fsend.at[i], recv_sem=frecv.at[i],
                device_id={"c": lax.rem(c + dc, 2), "tp": to}, device_id_type=MESH,
            )
        )
    for cp in finals:
        cp.start()
    fin[c, t] = fst[0, t]
    for cp in finals:
        cp.wait_recv()
    totals = []
    for k in range(2):
        total = fin[k, 0].astype(F32)
        for i in range(1, 4):
            total += fin[k, i].astype(F32)
        totals.append(total.astype(BF16))
    trow = iota((48, 32), 0)
    tcol = iota((48, 32), 1)
    want = 4 * (lax.rem(trow, 16) // 2) + trow // 16
    arranged = sum(dot(one_hot((lax.rem(trow, 2) == k) & (tcol == want)), totals[k]) for k in range(2))
    for j in range(3):
        mixed_o[j] = arranged[j * 16 : (j + 1) * 16].astype(BF16)

    for cp in finals:
        cp.wait_send()
    pltpu.make_async_remote_copy(
        src_ref=gath.at[0 : NZ - 1], dst_ref=gath.at[0 : NZ - 1], send_sem=gsend, recv_sem=nrecv, device_id=partner,
        device_id_type=MESH,
    ).wait_send()


def store(mixed, states, tail, mixed_o, states_o, tail_o, sem):
    copies = [
        pltpu.make_async_copy(src, dst, sem.at[i])
        for i, (src, dst) in enumerate(((states, states_o), (tail, tail_o), (mixed, mixed_o)))
    ]
    for cp in copies:
        cp.start()
    for cp in copies:
        cp.wait()


def local(
    tokens,
    input_norm_scale,
    head_input_matrix,
    output_gate_matrix,
    group_input_matrix,
    group_readout_matrix,
    step_size_matrix,
    step_size_bias,
    log_decay_rate,
    direct_path_weight,
    convolution_tap_weight,
    convolution_history_rows,
    per_proposal_states,
    accepted,
    proposal_extra_decay,
    group_norm_scale,
    output_projection_matrix,
):
    width = tokens.shape[2]
    heads = step_size_bias.shape[0]
    channels = heads * 64
    dma = pltpu.SemaphoreType.DMA
    any_space = pl.BlockSpec(memory_space=pl.ANY)
    vmem = pl.BlockSpec(memory_space=pltpu.VMEM)
    mixed, states, tail = pl.pallas_call(
        kernel,
        name="mixer",
        out_shape=(
            pltpu.VMEM((3, 16, 64), BF16),
            pltpu.VMEM((3, channels, 64), F32),
            pltpu.VMEM((6, 2, 1152), BF16),
        ),
        in_specs=[any_space] * 17,
        out_specs=(vmem, vmem, vmem),
        scratch_shapes=[
            pltpu.VMEM((3, width), BF16),
            pltpu.VMEM((1, width), F32),
            pltpu.VMEM((heads, width), BF16),
            pltpu.VMEM((1, heads), F32),
            pltpu.VMEM((1, heads), F32),
            pltpu.VMEM((1, heads), F32),
            pltpu.VMEM((4, 2, 1152), BF16),
            pltpu.VMEM((6, 2, 1152), BF16),
            pltpu.VMEM((3, channels, 64), F32),
            pltpu.VMEM((3, 1, heads), F32),
            pltpu.VMEM((1, channels), F32),
            pltpu.VMEM((64, channels), BF16),
            pltpu.VMEM((64, channels), BF16),
            pltpu.VMEM((CB * 128, BLK), BF16),
            pltpu.VMEM((NZ, 4, 128), BF16),
            pltpu.VMEM((NZ, 4, 128), BF16),
            pltpu.VMEM((NZ, 16, BLK), BF16),
            pltpu.VMEM((8, 4, 16, BLK), BF16),
            pltpu.VMEM((7, 16, BLK), BF16),
            pltpu.VMEM((7, 16, BLK), BF16),
            pltpu.VMEM((NZ, 16, GBLK), BF16),
            pltpu.VMEM((16, GBLK), BF16),
            pltpu.VMEM((2, 4, 32, 64), BF16),
            pltpu.VMEM((2, 4, 32, 64), BF16),
            pltpu.VMEM((channels, 128), BF16),
            dma((13 + len(PIECES),)),
            dma((len(PIECES) + 1,)),
            dma((len(PIECES) + 1,)),
            dma,
            dma((3,)),
            dma,
            dma((8,)),
            dma((7,)),
            dma((7,)),
            dma,
            dma((8,)),
            dma,
            dma((7,)),
            dma((7,)),
            pltpu.VMEM((8, 4, 128), BF16),
            pltpu.VMEM((7, 4, 128), BF16),
            dma((8,)),
            dma((8,)),
            dma((7,)),
            dma((7,)),
            pltpu.SemaphoreType.REGULAR((NZ,)),
            pltpu.SMEM((1,), jnp.int32),
            pltpu.VMEM((CLOSE, 4, 128), BF16),
            dma((CLOSE,)),
            dma((CLOSE,)),
        ],
        compiler_params=pltpu.CompilerParams(
            collective_id=0, has_side_effects=True, vmem_limit_bytes=56 * 1024 * 1024
        ),
    )(
        tokens,
        input_norm_scale.reshape(1, width),
        head_input_matrix,
        output_gate_matrix,
        group_input_matrix,
        group_readout_matrix,
        step_size_matrix.T,
        step_size_bias.reshape(1, heads),
        log_decay_rate.reshape(1, heads),
        direct_path_weight.reshape(1, heads),
        convolution_tap_weight,
        convolution_history_rows,
        per_proposal_states.reshape(3, channels, 64),
        accepted,
        proposal_extra_decay.transpose(1, 0, 2),
        group_norm_scale.reshape(1, channels),
        output_projection_matrix.T,
    )
    mixed, states, tail = pl.pallas_call(
        store,
        name="store",
        out_shape=(
            jax.ShapeDtypeStruct((3, 16, 64), BF16),
            jax.ShapeDtypeStruct((3, channels, 64), F32),
            jax.ShapeDtypeStruct((6, 2, 1152), BF16),
        ),
        in_specs=[pl.BlockSpec(memory_space=pltpu.VMEM)] * 3,
        out_specs=(any_space,) * 3,
        scratch_shapes=[dma((3,))],
    )(*(pltpu.with_memory_space_constraint(v, pltpu.VMEM) for v in (mixed, states, tail)))
    mixed = mixed.transpose(1, 0, 2)
    states = states.reshape(1, 3, heads, 64, 64)
    tail = tail[None]
    return mixed, states, tail


def solution(mesh):
    ring = mesh.shape["kv"] // 2
    assert ring == NZ and mesh.shape["tp"] == 4
    finer = Mesh(
        mesh.devices.reshape(mesh.shape["grp"], ring, 2, mesh.shape["tp"]),
        ("grp", "z", "c", "tp"),
    )
    return jax.shard_map(
        local,
        mesh=finer,
        in_specs=(
            P(GRP_KV, None, None),
            P(),
            P(KV, "tp"),
            P(KV, "tp"),
            P(KV, "tp"),
            P(KV, "tp"),
            P(None, "tp"),
            P("tp"),
            P("tp"),
            P("tp"),
            P(None, "tp", None),
            P(GRP_KV, None, "tp", None),
            P(GRP_KV, None, "tp", None, None),
            P(GRP_KV),
            P(GRP_KV, None, "tp"),
            P("tp"),
            P("tp", KV),
        ),
        out_specs=(
            P(("grp", "tp"), None, KV),
            P(GRP_KV, None, "tp", None, None),
            P(GRP_KV, None, "tp", None),
        ),
        check_vma=False,
    )
```
